256 devices in a mesh: grp: 2 (over y), st: 32 (over z, core), tp: 4 (over x).
Axes of the slice: x: 4, y: 2, z: 16, core: 2. Of those that a mesh axis runs over, the one named last changes fastest.
The devices are a block of a 4x16x16 slice.
Arguments:
- tokens: bfloat16 [32768, 2048], P(('grp', 'st')), parts along dimension 0, may hold values from -6 to 6
- owners: int32 [512, 4], P(('grp', 'st')), parts along dimension 0, may hold values from 0 to 31, all different within a row; in each aligned block of 8 rows (0 to 7, 8 to 15, ...) at most 2 rows name the same one
- entries: int32 [512, 4], P(('grp', 'st')), parts along dimension 0, may hold values from 0 to 15
- store: bfloat16 [1024, 64, 2048], P(('grp', 'st')), parts along dimension 0, may hold values from -600 to 600
- mixer_query_weight: bfloat16 [2048, 1024], P(None, 'tp'), may hold values from -0.125 to 0.125
- mixer_key_weight: bfloat16 [2048, 1024], P(None, 'tp'), may hold values from -0.125 to 0.125
- mixer_value_weight: bfloat16 [2048, 1024], P(None, 'tp'), may hold values from -0.125 to 0.125
- strength_weight: bfloat16 [2048, 8], P(None, 'tp'), may hold values from -0.125 to 0.125
- decay_weight: bfloat16 [2048, 8], P(None, 'tp'), may hold values from -0.125 to 0.125
- head_decay_rate: float32 [8], P('tp'), may hold values from 0.003 to 0.15
- extra_forgetting_exponent: float32 [32768, 8], P(('grp', 'st'), 'tp'), parts along dimension 0, may hold values from -0.7 to 0
- output_norm_gain: float32 [128], replicated, may hold values from 0.1 to 1.9
- retrieval_query_weight: bfloat16 [2048, 1024], P(None, 'tp'), may hold values from -0.125 to 0.125
- passage_key_weight: bfloat16 [2048, 1024], P(None, 'tp'), may hold values from -0.125 to 0.125
- passage_value_weight: bfloat16 [2048, 1024], P(None, 'tp'), may hold values from -0.125 to 0.125
- retrieval_gate_weight: bfloat16 [2048, 8], P(None, 'tp'), may hold values from -0.125 to 0.125
Outputs:
- mixed: bfloat16 [32768, 1024], P(('grp', 'st'), 'tp'), parts along dimension 0
The draws below stay inside these ranges and needn't reach their ends.
There are 2 independent parts, one for each index of `grp`. The reference program is written for one: setup_inputs(seed, part) draws one part's arguments, and reference() takes and returns one part's arrays. A program takes and returns all parts, laid end to end along the dimension named above; an argument that names none is the same for every part. Nothing has to cross between parts.
Inputs may be any that keep to these rules, and one draw needn't show every extreme that they name: `owners`: each row names 4 different values; the rows of one device name no value more than 2 times, a bound that some device reaches; every value is named by some row.
All inputs are finite; a program needn't handle non-finite values.
Results may differ from the reference program's by a relative error of at most 0.015.
The reference program's roundings to bfloat16 on the way count: a program that leaves them out, or rounds other values in their place, can miss the bound.
Values may be sent and summed in bfloat16 or wider, within the bound.
A program may use at most 128 MiB of HBM per device.

```python
import math
import jax
import jax.numpy as jnp
import numpy as np
from jax import lax

D = 2048
ATTENTION_GROUPS = 8
FEATURE_WIDTH = 128
STREAM_LENGTH = 512
PASS_DEV = 16
BLOCK_TOKENS = 64
PER_BLOCK = 4
PASS_LEN = 64
POSITIONS_ALL = 16384
BLK_DEV = 8
BLOCKS = 256
PASSAGES = 512
CAP = 2
N_ST = 32


def draw_store(key, part):
    base_key = jax.random.fold_in(key, 0)
    shape = (PASSAGES, PASS_LEN, D)
    values = jnp.clip(jax.random.normal(base_key, shape, jnp.float32), -6.0, 6.0)
    return values.astype(jnp.bfloat16)


def draw_extra_forgetting_exponent(key, part):
    where_key, depth_key = jax.random.split(key, 2)
    shape = (POSITIONS_ALL, ATTENTION_GROUPS)
    struck = jax.random.uniform(where_key, shape, jnp.float32) < 1.0 / 128.0
    depth = jnp.log(jax.random.uniform(depth_key, shape, jnp.float32, 0.5, 0.8))
    return jnp.where(struck, depth, 0.0).astype(jnp.float32)


def touch_ends(values, key, low, largest):
    longest = values.shape.index(max(values.shape))
    spots = []
    for shift in (0, 1):
        where = [jax.random.randint(jax.random.fold_in(key, axis), (), 0, length) for axis, length in enumerate(values.shape)]
        where[longest] = (where[longest] + shift) % values.shape[longest]
        spots.append(tuple(where))
    return values.at[spots[0]].set(low).at[spots[1]].set(largest)


def block_scale(rng, extent, cuts, least, top_value):
    loudness = 1.0
    for position, blocks in cuts:
        steps = jax.random.uniform(jax.random.fold_in(jax.random.fold_in(rng, 6), position), (blocks,), jnp.float32, least / len(cuts), top_value / len(cuts))
        loudness = loudness * jnp.repeat(jnp.exp(steps), extent[position] // blocks).reshape((-1,) + (1,) * (len(extent) - 1 - position))
    return loudness


def deal_out(key, own, number, rows, number_of, top, most, lean):
    sequence = jax.random.permutation(key, number_of)
    heavy_load, common = portions_of(number_of, rows * top, most, lean, True), portions_of(number_of, rows * top, most, lean, False)
    places = jnp.arange(number_of)

    def named(tallies, offset_by):
        used = int((tallies > 0).sum())
        fixed = max(1, used // 4)
        moved = fixed + (places - fixed + offset_by * (used - fixed)) % max(1, number_of - fixed)
        return jnp.zeros((number_of,), jnp.int32).at[sequence[jnp.where(places < fixed, places, moved)]].set(jnp.asarray(tallies, jnp.int32))

    tallies = jnp.where(number % 4 == 0, named(heavy_load, number // 4), named(common, number - number // 4 - 1))
    mixed = jax.random.permutation(jax.random.fold_in(own, 3), number_of)
    donor, taker = mixed[0:number_of // 2 * 2:2], mixed[1:number_of // 2 * 2:2]
    room = jnp.minimum(tallies[donor] - 1, most - tallies[taker]) // 2
    room = jnp.where((donor == sequence[0]) | (taker == sequence[0]) | (tallies[taker] == 0), 0, jnp.maximum(room, 0))
    moved = jax.random.randint(jax.random.fold_in(own, 4), (number_of // 2,), 0, 1 << 20) % (room + 1)
    tallies = tallies.at[donor].add(-moved).at[taker].add(moved)
    members = jnp.searchsorted(jnp.cumsum(tallies), jnp.arange(rows * top), side="right").astype(jnp.int32)
    listing = members.reshape(top, rows).T
    listing = listing[jax.random.permutation(jax.random.fold_in(own, 1), rows)]
    offset_by = jax.random.randint(jax.random.fold_in(own, 2), (rows, 1), 0, top)
    return jnp.take_along_axis(listing, (jnp.arange(top)[None, :] + offset_by) % top, axis=1)


def portions_of(number_of, total, bound, lean, full):
    loads = [(1 << 20) // math.isqrt(standing ** lean) + 1 for standing in range(1, number_of + 1)]
    largest = bound if full else min(bound, max(-(-total // number_of), total * loads[0] // sum(loads)))
    least = 1 if total - largest >= number_of - 1 else 0
    counts, rest = [largest] + [least] * (number_of - 1), total - largest - least * (number_of - 1)
    while rest > 0:
        candidates = [i for i in range(1, number_of) if counts[i] < largest] or [i for i in range(1, number_of) if counts[i] < bound]
        pool, remaining = sum([loads[i] for i in candidates]), rest
        for i in candidates:
            addition = min(bound - counts[i], max(1, remaining * loads[i] // pool), rest)
            counts[i] = counts[i] + addition
            rest = rest - addition
    return np.array(counts)


def scatter_about(stream_key, extent, deviation, reach, shards=(), kind=jnp.bfloat16):
    gain = block_scale(stream_key, extent, shards, -0.22, 0.18) if shards else 1.0
    values = jax.random.normal(stream_key, extent, jnp.float32) * deviation * gain
    return jnp.minimum(jnp.maximum(values, -reach), reach).astype(kind)


def setup_inputs(seed: int = 0, part: int = 0) -> dict:
    keys = jax.random.split(jax.random.key(seed), 17)
    own_keys = jax.random.split(jax.random.fold_in(keys[16], part), 17)
    tokens = scatter_about(own_keys[0], (POSITIONS_ALL, D), 1.0, 6.0, ((0, 32),))
    owners_keys = jax.random.split(jax.random.fold_in(own_keys[1], 1), BLOCKS // BLK_DEV)
    owners_turns = jax.random.permutation(jax.random.fold_in(own_keys[1], 3), BLOCKS // BLK_DEV)
    owners = jax.vmap(lambda own, number: deal_out(jax.random.fold_in(own_keys[1], 2), own, number, BLK_DEV, N_ST, PER_BLOCK, CAP, 2))(owners_keys, owners_turns).reshape((BLOCKS, PER_BLOCK))
    entries = touch_ends(jax.random.randint(own_keys[2], (BLOCKS, PER_BLOCK), 0, PASS_DEV), jax.random.fold_in(own_keys[2], 1), 0, PASS_DEV - 1).astype(jnp.int32)
    store = draw_store(jax.random.fold_in(jax.random.fold_in(keys[16], part), 71), part)
    mixer_query_weight = scatter_about(keys[4], (D, ATTENTION_GROUPS * FEATURE_WIDTH), D ** -0.5, 0.125, ((1, 4),))
    mixer_key_weight = scatter_about(keys[5], (D, ATTENTION_GROUPS * FEATURE_WIDTH), D ** -0.5, 0.125, ((1, 4),))
    mixer_value_weight = scatter_about(keys[6], (D, ATTENTION_GROUPS * FEATURE_WIDTH), D ** -0.5, 0.125, ((1, 4),))
    strength_weight = scatter_about(keys[7], (D, ATTENTION_GROUPS), D ** -0.5, 0.125, ((1, 4),))
    decay_weight = scatter_about(keys[8], (D, ATTENTION_GROUPS), D ** -0.5, 0.125, ((1, 4),))
    head_decay_rate = jnp.clip(jnp.exp(math.log(0.15) - 3.912023 * jax.random.uniform(keys[9], (ATTENTION_GROUPS,), jnp.float32) ** block_scale(keys[9], (ATTENTION_GROUPS,), ((0, 4),), -0.2, 0.2)), 0.003, 0.15)
    extra_forgetting_exponent = draw_extra_forgetting_exponent(jax.random.fold_in(jax.random.fold_in(keys[16], part), 71), part)
    output_norm_gain = jnp.clip(1.0 + 0.18 * jax.random.normal(keys[11], (FEATURE_WIDTH,), jnp.float32), 0.1, 1.9)
    retrieval_query_weight = scatter_about(keys[12], (D, ATTENTION_GROUPS * FEATURE_WIDTH), D ** -0.5, 0.125, ((1, 4),))
    passage_key_weight = scatter_about(keys[13], (D, ATTENTION_GROUPS * FEATURE_WIDTH), D ** -0.5, 0.125, ((1, 4),))
    passage_value_weight = scatter_about(keys[14], (D, ATTENTION_GROUPS * FEATURE_WIDTH), D ** -0.5, 0.125, ((1, 4),))
    retrieval_gate_weight = scatter_about(keys[15], (D, ATTENTION_GROUPS), D ** -0.5, 0.125, ((1, 4),))
    return {"tokens": tokens, "owners": owners, "entries": entries, "store": store, "mixer_query_weight": mixer_query_weight, "mixer_key_weight": mixer_key_weight, "mixer_value_weight": mixer_value_weight, "strength_weight": strength_weight, "decay_weight": decay_weight, "head_decay_rate": head_decay_rate, "extra_forgetting_exponent": extra_forgetting_exponent, "output_norm_gain": output_norm_gain, "retrieval_query_weight": retrieval_query_weight, "passage_key_weight": passage_key_weight, "passage_value_weight": passage_value_weight, "retrieval_gate_weight": retrieval_gate_weight}


eps = 1e-06

def matmul_high(left, right):
    return jnp.einsum('...ij,...jk->...ik', left, right, precision=lax.Precision.HIGHEST)

def unit_lower_inverse(strict_part):
    size = strict_part.shape[-1]
    ident = jnp.eye(size, dtype=jnp.float32)
    inverse = ident - strict_part
    power = strict_part
    for level in range(size.bit_length() - 2):
        power = matmul_high(power, power)
        inverse = matmul_high(inverse, ident + power)
    return inverse

def delta_rule(queries, keys_in, values_in, decay_logarithm, strength, block_slice):
    length, heads, width = queries.shape
    count = length // block_slice

    def split(array):
        return array.reshape(count, block_slice, heads, array.shape[-1]).transpose(0, 2, 1, 3)
    q_blk = split(queries)
    k_blk = split(keys_in)
    v_blk = split(values_in)
    decay_blk = decay_logarithm.reshape(count, block_slice, heads).transpose(0, 2, 1)
    beta_blk = strength.reshape(count, block_slice, heads).transpose(0, 2, 1)
    cumul = jnp.cumsum(decay_blk, axis=-1)
    lower = jnp.tril(jnp.ones((block_slice, block_slice), bool))
    strict = jnp.tril(jnp.ones((block_slice, block_slice), bool), -1)
    spread = cumul[..., :, None] - cumul[..., None, :]
    damping = jnp.where(lower, jnp.exp(jnp.where(lower, spread, 0.0)), 0.0)
    k_beta = k_blk * beta_blk[..., None]
    inner = jnp.where(strict, matmul_high(k_beta, jnp.swapaxes(k_blk, -1, -2)) * damping, 0.0)
    inverse = unit_lower_inverse(inner)
    fresh_base = matmul_high(inverse, v_blk * beta_blk[..., None])
    key_mix = matmul_high(inverse, k_beta * jnp.exp(cumul)[..., None])
    within = jnp.where(lower, matmul_high(q_blk, jnp.swapaxes(k_blk, -1, -2)) * damping, 0.0)
    q_decayed = q_blk * jnp.exp(cumul)[..., None]
    k_tail = k_blk * jnp.exp(cumul[..., -1:] - cumul)[..., None]
    carry_decay = jnp.exp(cumul[..., -1])

    def advance(state, pieces):
        q_part, k_part, base_part, mix_part, within_part, decay_part = pieces
        fresh = base_part - matmul_high(mix_part, state)
        result = matmul_high(q_part, state) + matmul_high(within_part, fresh)
        state = state * decay_part[:, None, None] + matmul_high(jnp.swapaxes(k_part, -1, -2), fresh)
        return (state, result)
    start = jnp.zeros((heads, width, values_in.shape[-1]), jnp.float32)
    final, outputs = lax.scan(advance, start, (q_decayed, k_tail, fresh_base, key_mix, within, carry_decay))
    return outputs.transpose(0, 2, 1, 3).reshape(length, heads, values_in.shape[-1])

def mixer_head_outputs(tokens, mixer_query_weight, mixer_key_weight, mixer_value_weight, strength_weight, decay_weight, head_decay_rate, extra_forgetting_exponent, output_norm_gain, block_slice):
    heads = head_decay_rate.shape[0]
    head_dim = output_norm_gain.shape[0]
    length = tokens.shape[0]

    def project(weight):
        rounded = jnp.dot(tokens, weight, preferred_element_type=jnp.float32).astype(jnp.bfloat16)
        return lax.optimization_barrier(rounded).astype(jnp.float32).reshape(length, heads, head_dim)

    def unit_rows(array):
        return array * lax.rsqrt(lax.optimization_barrier(jnp.sum(array * array, axis=-1, keepdims=True)) + eps)
    queries = unit_rows(project(mixer_query_weight)) * head_dim ** (-0.5)
    keys_in = unit_rows(project(mixer_key_weight))
    values_in = project(mixer_value_weight)
    strength = jax.nn.sigmoid(jnp.dot(tokens, strength_weight, preferred_element_type=jnp.float32))
    decay_logarithm = -head_decay_rate[None, :] * jax.nn.softplus(jnp.dot(tokens, decay_weight, preferred_element_type=jnp.float32)) + extra_forgetting_exponent
    recur = delta_rule(queries, keys_in, values_in, decay_logarithm, strength, block_slice)
    return recur * lax.rsqrt(lax.optimization_barrier(jnp.mean(recur * recur, axis=-1, keepdims=True)) + eps) * output_norm_gain

def reference(tokens, owners, entries, store, mixer_query_weight, mixer_key_weight, mixer_value_weight, strength_weight, decay_weight, head_decay_rate, extra_forgetting_exponent, output_norm_gain, retrieval_query_weight, passage_key_weight, passage_value_weight, retrieval_gate_weight):
    stream_group = tokens.reshape(N_ST, STREAM_LENGTH, D)
    forgetting_spikes = extra_forgetting_exponent.reshape(N_ST, STREAM_LENGTH, ATTENTION_GROUPS)

    def lone_stream(pair):
        return mixer_head_outputs(pair[0], mixer_query_weight, mixer_key_weight, mixer_value_weight, strength_weight, decay_weight, head_decay_rate, pair[1], output_norm_gain, BLOCK_TOKENS)
    rescaled_result = lax.map(lone_stream, (stream_group, forgetting_spikes)).reshape(POSITIONS_ALL, ATTENTION_GROUPS, FEATURE_WIDTH)
    flat_store = store.reshape(PASSAGES * PASS_LEN, D)
    pass_key = jnp.dot(flat_store, passage_key_weight, preferred_element_type=jnp.float32).astype(jnp.bfloat16).reshape(PASSAGES, PASS_LEN, ATTENTION_GROUPS * FEATURE_WIDTH)
    pass_value = jnp.dot(flat_store, passage_value_weight, preferred_element_type=jnp.float32).astype(jnp.bfloat16).reshape(PASSAGES, PASS_LEN, ATTENTION_GROUPS * FEATURE_WIDTH)
    passage = (owners.astype(jnp.int32) * PASS_DEV + entries.astype(jnp.int32)).astype(jnp.int32)
    keys_read = pass_key[passage].reshape(BLOCKS, PER_BLOCK * PASS_LEN, ATTENTION_GROUPS, FEATURE_WIDTH)
    values_read = pass_value[passage].reshape(BLOCKS, PER_BLOCK * PASS_LEN, ATTENTION_GROUPS, FEATURE_WIDTH)
    rquery = jnp.dot(tokens, retrieval_query_weight, preferred_element_type=jnp.float32).astype(jnp.bfloat16).reshape(BLOCKS, BLOCK_TOKENS, ATTENTION_GROUPS, FEATURE_WIDTH)
    scores = jnp.einsum('bqhd,bkhd->bhqk', rquery.astype(jnp.float32), keys_read.astype(jnp.float32)) * FEATURE_WIDTH ** (-0.5)
    peak = lax.optimization_barrier(jnp.max(scores, axis=-1, keepdims=True))
    expo = jnp.exp(scores - peak)
    weights = (expo / lax.optimization_barrier(jnp.sum(expo, axis=-1, keepdims=True))).astype(jnp.bfloat16)
    retrieved = jnp.einsum('bhqk,bkhd->bqhd', weights.astype(jnp.float32), values_read.astype(jnp.float32)).reshape(POSITIONS_ALL, ATTENTION_GROUPS, FEATURE_WIDTH)
    rgate = jax.nn.sigmoid(jnp.dot(tokens, retrieval_gate_weight, preferred_element_type=jnp.float32))
    mixed = rescaled_result + rgate[..., None] * retrieved
    return mixed.reshape(POSITIONS_ALL, ATTENTION_GROUPS * FEATURE_WIDTH).astype(jnp.bfloat16)
```

```python
import functools

import jax
import jax.numpy as jnp
from jax import lax
from jax.experimental import pallas as pl
from jax.experimental.pallas import tpu as pltpu
from jax.sharding import PartitionSpec as P

MESH = pl.DeviceIdType.MESH
EPS = 1e-06
NEVER = -1e30
BLOCK = 64
TILE = 128
NN = (((1,), (0,)), ((), ()))
NT = (((1,), (1,)), ((), ()))
TN = (((0,), (0,)), ((), ()))


def dot(left, right, dims=NN):
    return lax.dot_general(left, right, dims, preferred_element_type=jnp.float32)


def bdot(left, right, dims=NN):
    return dot(left.astype(jnp.bfloat16), right.astype(jnp.bfloat16), dims)


def rounded(array):
    return array.astype(jnp.bfloat16).astype(jnp.float32)


def kernel(
    chips,
    tok_h,
    store_h,
    wrq_h,
    wpk_h,
    wpv_h,
    wq_h,
    wk_h,
    wv_h,
    owners,
    entries,
    small_w,
    forget,
    rate,
    gain,
    out,
    tok,
    store,
    wts,
    qall,
    meta,
    smeta,
    held,
    kv,
    slot,
    slot_l,
    part,
    part_l,
    ret1,
    ret1_l,
    ret2,
    ret2_l,
    fac,
    qn,
    kn,
    vn,
    rows,
    cols,
    rgate,
    power,
    inverse,
    within,
    state,
    normed,
    load_sem,
    q_send,
    q_recv,
    r_send,
    r_recv,
    kv_send,
    kv_recv,
    sm_sem,
):
    far = chips // 2
    near = chips - 1 - far
    me = lax.axis_index("st")
    core = lax.rem(me, 2)
    chip = lax.div(me, 2)
    sign = 1 - 2 * core
    ahead = lax.rem(chip + sign + chips, chips) * 2 + core
    behind = lax.rem(chip - sign + chips, chips) * 2 + core
    peer = me + sign
    tiles = qall.shape[1] // 2
    heads = slot.shape[3]
    scale = TILE ** (-0.5)
    column = (me, peer)

    barrier = pltpu.get_barrier_semaphore()
    for other in (ahead, behind, peer):
        pl.semaphore_signal(barrier, inc=1, device_id={"st": other}, device_id_type=MESH)

    tok_rows = tok.shape[0] // tiles
    store_rows = store.shape[0] // tiles

    def load_w(index, ref):
        return pltpu.make_async_copy(ref, wts.at[index], load_sem.at[index])

    def load_tok(t):
        span = pl.ds(t * tok_rows, tok_rows)
        return pltpu.make_async_copy(tok_h.at[span], tok.at[span], load_sem.at[6 + t])

    def load_store(t):
        span = pl.ds(t * store_rows, store_rows)
        return pltpu.make_async_copy(
            store_h.at[span], store.at[span], load_sem.at[6 + tiles + t]
        )

    load_w(0, wrq_h).start()
    for t in range(tiles):
        load_tok(t).start()
    load_w(1, wpk_h).start()
    load_w(2, wpv_h).start()
    for t in range(tiles):
        load_store(t).start()
    load_w(3, wq_h).start()
    load_w(4, wk_h).start()
    load_w(5, wv_h).start()

    lane = lax.broadcasted_iota(jnp.int32, (8, TILE), 1)
    hit = jnp.zeros((8, TILE), jnp.int32)
    entry = jnp.zeros((8, TILE), jnp.int32)
    for i in range(owners.shape[1]):
        same = owners[:, i : i + 1] == lane
        hit = jnp.where(same, 1, hit)
        entry = jnp.where(same, entries[:, i : i + 1], entry)
    count = jnp.zeros((1, TILE), jnp.int32)
    picks = [jnp.zeros((1, TILE), jnp.int32) for _ in range(4)]
    ranks = []
    for b in range(8):
        here = hit[b : b + 1, :]
        ranks.append(jnp.where(here > 0, jnp.minimum(count, 2), 2))
        for r in range(2):
            chosen = (here > 0) & (count == r)
            picks[2 * r] = jnp.where(chosen, b, picks[2 * r])
            picks[2 * r + 1] = jnp.where(chosen, entry[b : b + 1, :], picks[2 * r + 1])
        count = count + here
    for b in range(8):
        row = ranks[b]
        if b < 4:
            row = row + 4 * picks[b]
        meta[0, b : b + 1, :] = row

    def q_copy(way, k, c):
        if way == 0:
            source, target, device = k - 1, k, ahead
        else:
            source, target, device = jnp.where(k == 1, 0, far + k - 1), far + k, behind
        if c == tiles:
            src, dst = meta.at[source], meta.at[target]
        else:
            src, dst = qall.at[source, pl.ds(2 * c, 2)], qall.at[target, pl.ds(2 * c, 2)]
        return pltpu.make_async_remote_copy(
            src_ref=src,
            dst_ref=dst,
            send_sem=q_send.at[way, k - 1, c],
            recv_sem=q_recv.at[way, k - 1, c],
            device_id={"st": device},
            device_id_type=MESH,
        )

    def r_copy(way, i, c):
        ref, ref_l = ((ret1, ret1_l), (ret2, ret2_l))[way]
        if c == tiles:
            src, dst = ref_l.at[i], ref_l.at[i + 1]
        else:
            src, dst = ref.at[i, c], ref.at[i + 1, c]
        return pltpu.make_async_remote_copy(
            src_ref=src,
            dst_ref=dst,
            send_sem=r_send.at[way, i, c],
            recv_sem=r_recv.at[way, i, c],
            device_id={"st": (behind, ahead)[way]},
            device_id_type=MESH,
        )

    def kv_copy(which):
        return pltpu.make_async_remote_copy(
            src_ref=kv.at[0, which],
            dst_ref=kv.at[1, which],
            send_sem=kv_send.at[which],
            recv_sem=kv_recv.at[which],
            device_id={"st": peer},
            device_id_type=MESH,
        )

    def sm_copy(way, index, slot_index):
        return pltpu.make_async_copy(
            meta.at[index], smeta.at[way, slot_index], sm_sem.at[way, slot_index]
        )

    load_w(0, wrq_h).wait()
    pl.semaphore_wait(barrier, 3)
    for way in range(2):
        q_copy(way, 1, tiles).start()
    for t in range(tiles):
        load_tok(t).wait()
        own = dot(tok[t * tok_rows : (t + 1) * tok_rows, :], wts[0]).astype(jnp.bfloat16)
        qall[0, 2 * t : 2 * t + 2] = own.reshape(2, BLOCK, own.shape[1])
        if t:
            for way in range(2):
                q_copy(way, 1, t - 1).start()

    slot[:, :, 2] = jnp.zeros(slot.shape[:2] + slot.shape[3:], slot.dtype)
    slot_l[:, :, 2] = jnp.full(slot_l.shape[:2] + slot_l.shape[3:], NEVER, jnp.float32)
    state[...] = jnp.zeros_like(state)
    for way in range(2):
        q_copy(way, 1, tiles - 1).start()

    load_w(1, wpk_h).wait()
    load_w(2, wpv_h).wait()
    group = kv.shape[2] // tiles

    def project_passages(t, carry):
        load_store(t).wait()
        piece = store[pl.ds(t * store_rows, store_rows), :]
        for which in range(2):
            made = dot(piece, wts[1 + which]).astype(jnp.bfloat16)
            kv[0, which, pl.ds(t * group, group)] = made.reshape(group, BLOCK, made.shape[1])
        return carry

    lax.fori_loop(0, tiles, project_passages, 0)

    def forward(k, c):
        last_far = isinstance(k, int) and k >= far
        q_copy(0, k, c).wait_recv()
        if not last_far:
            q_copy(0, k + 1, c).start()
            q_copy(1, k, c).wait_recv()

            @pl.when(k < near)
            def _():
                q_copy(1, k + 1, c).start()

    row_i = lax.broadcasted_iota(jnp.int32, (TILE, TILE), 0)
    col_i = lax.broadcasted_iota(jnp.int32, (TILE, TILE), 1)
    first_half = lax.broadcasted_iota(jnp.int32, (1, TILE), 1) < BLOCK

    def project_tokens(t):
        piece = tok[t * tok_rows : (t + 1) * tok_rows, :]
        for index, ref in ((3, qn), (4, kn), (5, vn)):
            made = rounded(dot(piece, wts[index]))
            for h in range(heads):
                one = made[:, h * TILE : (h + 1) * TILE]
                if index < 5:
                    one = one * lax.rsqrt(jnp.sum(one * one, axis=1, keepdims=True) + EPS)
                if index == 3:
                    one = one * scale
                ref[t, h] = one
        gates = jnp.transpose(dot(piece, small_w[...], NT))
        beta = jax.nn.sigmoid(gates[0:2, :])
        raw = gates[2:4, :]
        soft = jnp.maximum(raw, 0.0) + jnp.log1p(jnp.exp(-jnp.abs(raw)))
        cumul = -rate[...] * soft + forget[t]
        spot = lax.broadcasted_iota(jnp.int32, cumul.shape, 1)
        shift = 1
        while shift < TILE:
            cumul = cumul + jnp.where(spot >= shift, pltpu.roll(cumul, shift, 1), 0.0)
            shift *= 2
        tail = jnp.exp(cumul[:, TILE - 1 : TILE] - cumul)
        lines = jnp.concatenate([cumul, jnp.exp(cumul), tail, beta], axis=0)
        rows[t] = lines
        cols[t] = jnp.transpose(lines)
        rgate[t] = jax.nn.sigmoid(gates[4:6, :])

    def attend(way, parity, j, r):
        block = lax.shift_right_logical(smeta[way, parity, 2 * r, column[j]], 2)
        passage = lax.shift_right_logical(smeta[way, parity, 2 * r + 1, column[j]], 2)
        query = held[way, block]
        query = jnp.concatenate([query, query], axis=0)
        keys = kv[j, 0, passage]
        values = kv[j, 1, passage]
        for h in range(heads):
            span = slice(h * TILE, (h + 1) * TILE)
            scores = dot(keys[:, span], query[:, span], NT) * scale
            peak = jnp.max(scores, axis=0, keepdims=True)
            expo = jnp.exp(scores - peak)
            total = jnp.sum(expo, axis=0, keepdims=True)
            weights = (expo / total).astype(jnp.bfloat16)
            slot[way, j, r, h] = dot(values[:, span], weights, TN)
            slot_l[way, j, r, h] = jnp.broadcast_to(peak + jnp.log(total), (8, TILE))

    def assemble(s, way, parity):
        for t in range(tiles):
            picks = [
                [smeta[way, parity, 2 * t + half, column[j]] & 3 for half in range(2)]
                for j in range(2)
            ]
            for h in range(heads):
                logs = [
                    jnp.where(
                        first_half,
                        slot_l[way, j, picks[j][0], h, 0:1, :],
                        slot_l[way, j, picks[j][1], h, 0:1, :],
                    )
                    for j in range(2)
                ]
                peak = jnp.maximum(logs[0], logs[1])
                shares = [jnp.exp(one - peak) for one in logs]
                total = shares[0] + shares[1]
                made = 0.0
                for j in range(2):
                    both = jnp.where(
                        first_half,
                        slot[way, j, picks[j][0], h],
                        slot[way, j, picks[j][1], h],
                    )
                    made = made + both * (shares[j] / total)
                part[s, t, h * TILE : (h + 1) * TILE, :] = made
                part_l[s, h * tiles + t : h * tiles + t + 1, :] = peak + jnp.log(total)

    def delta(t, stage):
        ident = jnp.where(row_i == col_i, 1.0, 0.0)
        for h in range(heads):
            if stage == 0:
                lower = row_i >= col_i
                spread = cols[t, :, h : h + 1] - rows[t, h : h + 1, :]
                damping = jnp.where(lower, jnp.exp(jnp.where(lower, spread, 0.0)), 0.0)
                keys = kn[t, h]
                k_beta = keys * cols[t, :, 6 + h : 7 + h]
                inner = jnp.where(row_i > col_i, bdot(k_beta, keys, NT) * damping, 0.0)
                within[h] = jnp.where(lower, bdot(qn[t, h], keys, NT) * damping, 0.0)
                power[h] = inner
                inverse[h] = ident - inner
            elif stage < 3:
                value, made = power[h], inverse[h]
                for _ in range(3):
                    value = bdot(value, value)
                    made = bdot(made, ident + value)
                power[h] = value
                inverse[h] = made
            else:
                beta = cols[t, :, 6 + h : 7 + h]
                grown = cols[t, :, 2 + h : 3 + h]
                keys = kn[t, h]
                made = inverse[h]
                now = state[h]
                base = bdot(made, vn[t, h] * beta)
                mix = bdot(made, keys * beta * grown)
                fresh = base - bdot(mix, now)
                result = bdot(qn[t, h] * grown, now) + bdot(within[h], fresh)
                tail = keys * cols[t, :, 4 + h : 5 + h]
                state[h] = now * grown[TILE - 1 : TILE, :] + bdot(tail, fresh, TN)
                spread = jnp.mean(result * result, axis=1, keepdims=True)
                normed[t, h] = result * lax.rsqrt(spread + EPS) * gain[...]

    for which in range(2):
        kv_copy(which).start()
    for way in range(2):
        q_copy(way, 1, tiles).wait_recv()
        q_copy(way, 2, tiles).start()
        sm_copy(way, (1, far + 1)[way], 1).start()
    for c in range(tiles):
        forward(1, c)
        if c == 0:
            for index, ref in ((3, wq_h), (4, wk_h), (5, wv_h)):
                load_w(index, ref).wait()
        project_tokens(c)
    for which in range(2):
        kv_copy(which).wait_recv()

    def hop(k, carry):
        parity = lax.rem(k, 2)
        before = 1 - parity
        forward(k, tiles)
        for way in range(2):
            sm_copy(way, (k, far + k)[way], parity).start()
        for way in range(2):
            sm_copy(way, (k - 1, far + k - 1)[way], before).wait()
        for way in range(2):
            held[way] = qall[(k - 1, far + k - 1)[way]]
        for c in range(tiles):
            forward(k, c)
            for way in range(2):
                attend(way, before, c // 2, c % 2)
        for way in range(2):
            assemble((k - 1, far + k - 1)[way], way, before)
        return carry

    lax.fori_loop(2, near + 1, hop, 0)

    def whole(s, way, parity):
        held[way] = qall[s]
        for c in range(tiles):
            attend(way, parity, c // 2, c % 2)
        assemble(s, way, parity)

    def r_begin(way, s):
        ref, ref_l = ((ret1, ret1_l), (ret2, ret2_l))[way]
        ref_l[0] = part_l[s]
        for t in range(tiles):
            ref[0, t] = part[s, t].astype(jnp.bfloat16)
        for c in (tiles,) + tuple(range(tiles)):
            r_copy(way, 0, c).start()

    last = near % 2
    for way in range(2):
        sm_copy(way, (near, far + near)[way], last).wait()
    whole(far + near, 1, last)
    r_begin(1, far + near)
    q_copy(0, far, tiles).wait_recv()
    sm_copy(0, far, 1 - last).start()
    sm_copy(1, 0, 1 - last).start()
    for c in range(tiles):
        q_copy(0, far, c).wait_recv()
    sm_copy(0, far, 1 - last).wait()
    whole(far, 0, 1 - last)
    r_begin(0, far)
    whole(near, 0, last)
    sm_copy(1, 0, 1 - last).wait()
    whole(0, 1, 1 - last)

    def meet_logs(way, i, s):
        ref_l = (ret1_l, ret2_l)[way]
        r_copy(way, i - 1, tiles).wait_recv()
        theirs, mine = ref_l[i], part_l[s]
        peak = jnp.maximum(theirs, mine)
        shares = jnp.exp(theirs - peak), jnp.exp(mine - peak)
        total = shares[0] + shares[1]
        fac[way, 0] = shares[0] / total
        fac[way, 1] = shares[1] / total
        ref_l[i] = peak + jnp.log(total)

    def meet(way, i, s, t):
        ref = (ret1, ret2)[way]
        r_copy(way, i - 1, t).wait_recv()
        for h in range(heads):
            span = slice(h * TILE, (h + 1) * TILE)
            line = slice(h * tiles + t, h * tiles + t + 1)
            made = ref[i, t, span, :].astype(jnp.float32) * fac[way, 0, line, :]
            made = made + part[s, t, span, :] * fac[way, 1, line, :]
            ref[i, t, span, :] = made.astype(jnp.bfloat16)

    def back(i, carry):
        pair = far - i, far + near - i
        for way in range(2):
            meet_logs(way, i, pair[way])
        for c in range(tiles):
            for way in range(2):
                meet(way, i, pair[way], c)
            for way in range(2):
                if c == 0:
                    r_copy(way, i, tiles).start()
                r_copy(way, i, c).start()

            @pl.when(i <= tiles)
            def _():
                delta(i - 1, c)

        return carry

    lax.fori_loop(1, near, back, 0)
    meet_logs(0, near, far - near)
    for c in range(tiles):
        meet(0, near, far - near, c)
        if c == 0:
            r_copy(0, near, tiles).start()
        else:
            r_copy(0, near, c - 1).start()
    r_copy(1, near - 1, tiles).wait_recv()
    r_copy(0, near, tiles - 1).start()

    r_copy(0, far - 1, tiles).wait_recv()
    logs = part_l[0], ret1_l[far], ret2_l[near]
    peak = jnp.maximum(jnp.maximum(logs[0], logs[1]), logs[2])
    shares = [jnp.exp(one - peak) for one in logs]
    total = shares[0] + shares[1] + shares[2]
    shares = [one / total for one in shares]
    for t in range(tiles):
        r_copy(1, near - 1, t).wait_recv()
        r_copy(0, far - 1, t).wait_recv()
        for h in range(heads):
            span = slice(h * TILE, (h + 1) * TILE)
            line = slice(h * tiles + t, h * tiles + t + 1)
            made = part[0, t, span, :] * shares[0][line, :]
            made = made + ret1[far, t, span, :].astype(jnp.float32) * shares[1][line, :]
            made = made + ret2[near, t, span, :].astype(jnp.float32) * shares[2][line, :]
            made = jnp.transpose(made * rgate[t, h : h + 1, :])
            out[t * TILE : (t + 1) * TILE, span] = (normed[t, h] + made).astype(out.dtype)

    for which in range(2):
        kv_copy(which).wait_send()
    for way in range(2):
        hops = (far, near)[way]

        def drain(i, carry, way=way):
            for c in range(tiles + 1):
                q_copy(way, i + 1, c).wait_send()
                r_copy(way, i, c).wait_send()
            return carry

        lax.fori_loop(0, hops, drain, 0)


def per_device(
    tokens,
    owners,
    entries,
    store,
    mixer_query_weight,
    mixer_key_weight,
    mixer_value_weight,
    strength_weight,
    decay_weight,
    head_decay_rate,
    extra_forgetting_exponent,
    output_norm_gain,
    retrieval_query_weight,
    passage_key_weight,
    passage_value_weight,
    retrieval_gate_weight,
):
    heads = head_decay_rate.shape[0]
    length, model = tokens.shape
    width = mixer_query_weight.shape[1]
    blocks = owners.shape[0]
    passages, passage_rows = store.shape[:2]
    tiles = length // TILE
    chips = lax.axis_size("st") // 2
    far = chips // 2
    near = chips - 1 - far
    flat_store = store.reshape(passages * passage_rows, model)
    small_w = jnp.concatenate(
        [
            strength_weight.T,
            decay_weight.T,
            retrieval_gate_weight.T,
            jnp.zeros((8 - 3 * heads, model), tokens.dtype),
        ],
        axis=0,
    )
    forget = extra_forgetting_exponent.reshape(tiles, TILE, heads).transpose(0, 2, 1)
    rate = jnp.broadcast_to(head_decay_rate[:, None], (heads, TILE))
    any_spec = pl.BlockSpec(memory_space=pl.ANY)
    vmem_spec = pl.BlockSpec(memory_space=pltpu.VMEM)
    f32, bf16 = jnp.float32, jnp.bfloat16
    square = (TILE, TILE)
    return pl.pallas_call(
        functools.partial(kernel, chips),
        out_shape=jax.ShapeDtypeStruct((length, width), bf16),
        in_specs=[any_spec] * 8 + [vmem_spec] * 6,
        out_specs=vmem_spec,
        scratch_shapes=[
            pltpu.VMEM((length, model), bf16),
            pltpu.VMEM((passages * passage_rows, model), bf16),
            pltpu.VMEM((6, model, width), bf16),
            pltpu.VMEM((chips, blocks, BLOCK, width), bf16),
            pltpu.VMEM((chips, 8, TILE), jnp.int32),
            pltpu.SMEM((2, 2, 8, TILE), jnp.int32),
            pltpu.VMEM((2, blocks, BLOCK, width), bf16),
            pltpu.VMEM((2, 2, passages, passage_rows, width), bf16),
            pltpu.VMEM((2, 2, 3, heads) + square, f32),
            pltpu.VMEM((2, 2, 3, heads, 8, TILE), f32),
            pltpu.VMEM((chips, tiles, width, TILE), f32),
            pltpu.VMEM((chips, heads * tiles, TILE), f32),
            pltpu.VMEM((far + 1, tiles, width, TILE), bf16),
            pltpu.VMEM((far + 1, heads * tiles, TILE), f32),
            pltpu.VMEM((near + 1, tiles, width, TILE), bf16),
            pltpu.VMEM((near + 1, heads * tiles, TILE), f32),
            pltpu.VMEM((2, 2, heads * tiles, TILE), f32),
            pltpu.VMEM((tiles, heads) + square, f32),
            pltpu.VMEM((tiles, heads) + square, f32),
            pltpu.VMEM((tiles, heads) + square, f32),
            pltpu.VMEM((tiles, 8, TILE), f32),
            pltpu.VMEM((tiles, TILE, 8), f32),
            pltpu.VMEM((tiles, heads, TILE), f32),
            pltpu.VMEM((heads,) + square, f32),
            pltpu.VMEM((heads,) + square, f32),
            pltpu.VMEM((heads,) + square, f32),
            pltpu.VMEM((heads,) + square, f32),
            pltpu.VMEM((tiles, heads) + square, f32),
            pltpu.SemaphoreType.DMA((6 + 2 * tiles,)),
            pltpu.SemaphoreType.DMA((2, far, tiles + 1)),
            pltpu.SemaphoreType.DMA((2, far, tiles + 1)),
            pltpu.SemaphoreType.DMA((2, far, tiles + 1)),
            pltpu.SemaphoreType.DMA((2, far, tiles + 1)),
            pltpu.SemaphoreType.DMA((2,)),
            pltpu.SemaphoreType.DMA((2,)),
            pltpu.SemaphoreType.DMA((2, 2)),
        ],
        compiler_params=pltpu.CompilerParams(
            collective_id=0, has_side_effects=True, vmem_limit_bytes=60 * 1024 * 1024
        ),
    )(
        tokens,
        flat_store,
        retrieval_query_weight,
        passage_key_weight,
        passage_value_weight,
        mixer_query_weight,
        mixer_key_weight,
        mixer_value_weight,
        owners,
        entries,
        small_w,
        forget,
        rate,
        output_norm_gain[None, :],
    )


def solution(mesh):
    return jax.shard_map(
        per_device,
        mesh=mesh,
        in_specs=(
            P(("grp", "st"), None),
            P(("grp", "st"), None),
            P(("grp", "st"), None),
            P(("grp", "st"), None, None),
            P(None, "tp"),
            P(None, "tp"),
            P(None, "tp"),
            P(None, "tp"),
            P(None, "tp"),
            P("tp"),
            P(("grp", "st"), "tp"),
            P(),
            P(None, "tp"),
            P(None, "tp"),
            P(None, "tp"),
            P(None, "tp"),
        ),
        out_specs=P(("grp", "st"), "tp"),
        check_vma=False,
    )
```

```python
import functools

import jax
import jax.numpy as jnp
from jax import lax
from jax.experimental import pallas as pl
from jax.experimental.pallas import tpu as pltpu
from jax.sharding import PartitionSpec as P

MESH = pl.DeviceIdType.MESH
EPS = 1e-06
NEVER = -1e30
BLOCK = 64
TILE = 128
NN = (((1,), (0,)), ((), ()))
NT = (((1,), (1,)), ((), ()))
TN = (((0,), (0,)), ((), ()))


def dot(left, right, dims=NN):
    return lax.dot_general(left, right, dims, preferred_element_type=jnp.float32)


def bdot(left, right, dims=NN):
    return dot(left.astype(jnp.bfloat16), right.astype(jnp.bfloat16), dims)


def rounded(array):
    return array.astype(jnp.bfloat16).astype(jnp.float32)


def kernel(
    chips,
    tok_h,
    store_h,
    wrq_h,
    wpk_h,
    wpv_h,
    wq_h,
    wk_h,
    wv_h,
    owners_h,
    entries_h,
    strength_h,
    decay_h,
    gate_h,
    forget_h,
    rate_h,
    gain_h,
    out,
    owners,
    entries,
    strength,
    decay,
    gate,
    forget,
    rate,
    gain,
    tok,
    store,
    wts,
    qall,
    meta,
    smeta,
    held,
    kv,
    slot,
    slot_l,
    part,
    part_l,
    ret1,
    ret1_l,
    ret2,
    ret2_l,
    fac,
    qn,
    kn,
    vn,
    rows,
    cols,
    rgate,
    power,
    inverse,
    within,
    state,
    normed,
    load_sem,
    q_send,
    q_recv,
    r_send,
    r_recv,
    kv_send,
    kv_recv,
    sm_sem,
    in_sem,
):
    far = chips // 2
    near = chips - 1 - far
    me = lax.axis_index("st")
    core = lax.rem(me, 2)
    chip = lax.div(me, 2)
    sign = 1 - 2 * core
    ahead = lax.rem(chip + sign + chips, chips) * 2 + core
    behind = lax.rem(chip - sign + chips, chips) * 2 + core
    peer = me + sign
    tiles = qall.shape[1] // 2
    heads = slot.shape[3]
    scale = TILE ** (-0.5)
    column = (me, peer)
    members = 2 * chips

    barrier = pltpu.get_barrier_semaphore()
    for other in (ahead, behind, peer):
        pl.semaphore_signal(barrier, inc=1, device_id={"st": other}, device_id_type=MESH)

    tok_rows = tok.shape[0] // tiles
    store_rows = store.shape[0] // tiles

    def load_w(index, ref):
        return pltpu.make_async_copy(ref, wts.at[index], load_sem.at[index])

    def load_tok(t):
        span = pl.ds(t * tok_rows, tok_rows)
        return pltpu.make_async_copy(tok_h.at[span], tok.at[span], load_sem.at[6 + t])

    def load_store(t):
        span = pl.ds(t * store_rows, store_rows)
        return pltpu.make_async_copy(
            store_h.at[span], store.at[span], load_sem.at[6 + tiles + t]
        )

    small = [
        pltpu.make_async_copy(src, dst, in_sem.at[index])
        for index, (src, dst) in enumerate(
            (
                (owners_h, owners),
                (entries_h, entries),
                (strength_h, strength),
                (decay_h, decay),
                (gate_h, gate),
                (forget_h, forget),
                (rate_h, rate),
                (gain_h, gain),
            )
        )
    ]
    for copy in small[:2]:
        copy.start()
    load_w(0, wrq_h).start()
    for t in range(tiles):
        load_tok(t).start()
    for copy in small[2:]:
        copy.start()
    load_w(1, wpk_h).start()
    load_w(2, wpv_h).start()
    for t in range(tiles):
        load_store(t).start()
    load_w(3, wq_h).start()
    load_w(4, wk_h).start()
    load_w(5, wv_h).start()

    lane = lax.broadcasted_iota(jnp.int32, (1, TILE), 1)
    count = jnp.zeros((1, TILE), jnp.int32)
    picks = [jnp.zeros((1, TILE), jnp.int32) for _ in range(4)]
    ranks = []
    for copy in small[:2]:
        copy.wait()
    for b in range(8):
        hit = jnp.zeros((1, TILE), jnp.int32)
        entry = jnp.zeros((1, TILE), jnp.int32)
        for i in range(owners.shape[0]):
            same = lane == owners[i, b]
            hit = jnp.where(same, 1, hit)
            entry = jnp.where(same, entries[i, b], entry)
        ranks.append(jnp.where(hit > 0, jnp.minimum(count, 2), 2))
        for r in range(2):
            chosen = (hit > 0) & (count == r)
            picks[2 * r] = jnp.where(chosen, b, picks[2 * r])
            picks[2 * r + 1] = jnp.where(chosen, entry, picks[2 * r + 1])
        count = count + hit
    for b in range(8):
        row = ranks[b]
        if b < 4:
            row = jnp.where(lane < members, row, pltpu.roll(picks[b], members, 1))
        meta[0, b : b + 1, :] = row

    def q_copy(way, k, c):
        if way == 0:
            source, target, device = k - 1, k, ahead
        else:
            source, target, device = jnp.where(k == 1, 0, far + k - 1), far + k, behind
        if c == tiles:
            src, dst = meta.at[source], meta.at[target]
        else:
            src, dst = qall.at[source, pl.ds(2 * c, 2)], qall.at[target, pl.ds(2 * c, 2)]
        return pltpu.make_async_remote_copy(
            src_ref=src,
            dst_ref=dst,
            send_sem=q_send.at[way, k - 1, c],
            recv_sem=q_recv.at[way, k - 1, c],
            device_id={"st": device},
            device_id_type=MESH,
        )

    def r_copy(way, i, c):
        ref, ref_l = ((ret1, ret1_l), (ret2, ret2_l))[way]
        if c == tiles:
            src, dst = ref_l.at[i], ref_l.at[i + 1]
        else:
            src, dst = ref.at[i, c], ref.at[i + 1, c]
        return pltpu.make_async_remote_copy(
            src_ref=src,
            dst_ref=dst,
            send_sem=r_send.at[way, i, c],
            recv_sem=r_recv.at[way, i, c],
            device_id={"st": (behind, ahead)[way]},
            device_id_type=MESH,
        )

    def kv_copy(which):
        return pltpu.make_async_remote_copy(
            src_ref=kv.at[0, which],
            dst_ref=kv.at[1, which],
            send_sem=kv_send.at[which],
            recv_sem=kv_recv.at[which],
            device_id={"st": peer},
            device_id_type=MESH,
        )

    def sm_copy(way, index, slot_index):
        return pltpu.make_async_copy(
            meta.at[index], smeta.at[way, slot_index], sm_sem.at[way, slot_index]
        )

    load_w(0, wrq_h).wait()
    pl.semaphore_wait(barrier, 3)
    for way in range(2):
        q_copy(way, 1, tiles).start()
    for t in range(tiles):
        load_tok(t).wait()
        own = dot(tok[t * tok_rows : (t + 1) * tok_rows, :], wts[0]).astype(jnp.bfloat16)
        qall[0, 2 * t : 2 * t + 2] = own.reshape(2, BLOCK, own.shape[1])
        if t:
            for way in range(2):
                q_copy(way, 1, t - 1).start()

    slot[:, :, 2] = jnp.zeros(slot.shape[:2] + slot.shape[3:], slot.dtype)
    slot_l[:, :, 2] = jnp.full(slot_l.shape[:2] + slot_l.shape[3:], NEVER, jnp.float32)
    state[...] = jnp.zeros_like(state)
    for way in range(2):
        q_copy(way, 1, tiles - 1).start()

    load_w(1, wpk_h).wait()
    load_w(2, wpv_h).wait()
    group = kv.shape[2] // tiles

    def project_passages(t, carry):
        load_store(t).wait()
        piece = store[pl.ds(t * store_rows, store_rows), :]
        for which in range(2):
            made = dot(piece, wts[1 + which]).astype(jnp.bfloat16)
            kv[0, which, pl.ds(t * group, group)] = made.reshape(group, BLOCK, made.shape[1])
        return carry

    lax.fori_loop(0, tiles, project_passages, 0)

    def forward(k, c):
        last_far = isinstance(k, int) and k >= far
        q_copy(0, k, c).wait_recv()
        if not last_far:
            q_copy(0, k + 1, c).start()
            q_copy(1, k, c).wait_recv()

            @pl.when(k < near)
            def _():
                q_copy(1, k + 1, c).start()

    row_i = lax.broadcasted_iota(jnp.int32, (TILE, TILE), 0)
    col_i = lax.broadcasted_iota(jnp.int32, (TILE, TILE), 1)
    first_half = lax.broadcasted_iota(jnp.int32, (1, TILE), 1) < BLOCK

    def project_tokens(t):
        rates = jnp.where(
            lax.broadcasted_iota(jnp.int32, (heads, TILE), 0) == 0, rate[0:1, 0:1], rate[0:1, 1:2]
        )
        piece = tok[t * tok_rows : (t + 1) * tok_rows, :]
        for index, ref in ((3, qn), (4, kn), (5, vn)):
            made = rounded(dot(piece, wts[index]))
            for h in range(heads):
                one = made[:, h * TILE : (h + 1) * TILE]
                if index < 5:
                    one = one * lax.rsqrt(jnp.sum(one * one, axis=1, keepdims=True) + EPS)
                if index == 3:
                    one = one * scale
                ref[t, h] = one
        small_w = jnp.concatenate(
            [strength[...], decay[...], gate[...], jnp.zeros((2, tok.shape[1]), tok.dtype)], axis=0
        )
        gates = jnp.transpose(dot(piece, small_w, NT))
        beta = jax.nn.sigmoid(gates[0:2, :])
        raw = gates[2:4, :]
        soft = jnp.maximum(raw, 0.0) + jnp.log1p(jnp.exp(-jnp.abs(raw)))
        cumul = -rates * soft + forget[t]
        spot = lax.broadcasted_iota(jnp.int32, cumul.shape, 1)
        shift = 1
        while shift < TILE:
            cumul = cumul + jnp.where(spot >= shift, pltpu.roll(cumul, shift, 1), 0.0)
            shift *= 2
        tail = jnp.exp(cumul[:, TILE - 1 : TILE] - cumul)
        lines = jnp.concatenate([cumul, jnp.exp(cumul), tail, beta], axis=0)
        rows[t] = lines
        cols[t] = jnp.transpose(lines)
        rgate[t] = jax.nn.sigmoid(gates[4:6, :])

    def attend(way, parity, j, r):
        block = smeta[way, parity, 2 * r, column[j] + members]
        passage = smeta[way, parity, 2 * r + 1, column[j] + members]
        query = held[way, block]
        query = jnp.concatenate([query, query], axis=0)
        keys = kv[j, 0, passage]
        values = kv[j, 1, passage]
        for h in range(heads):
            span = slice(h * TILE, (h + 1) * TILE)
            scores = dot(keys[:, span], query[:, span], NT) * scale
            peak = jnp.max(scores, axis=0, keepdims=True)
            expo = jnp.exp(scores - peak)
            total = jnp.sum(expo, axis=0, keepdims=True)
            weights = (expo / total).astype(jnp.bfloat16)
            slot[way, j, r, h] = dot(values[:, span], weights, TN)
            slot_l[way, j, r, h] = jnp.broadcast_to(peak + jnp.log(total), (8, TILE))

    def assemble(s, way, parity):
        for t in range(tiles):
            picks = [
                [smeta[way, parity, 2 * t + half, column[j]] for half in range(2)]
                for j in range(2)
            ]
            for h in range(heads):
                logs = [
                    jnp.where(
                        first_half,
                        slot_l[way, j, picks[j][0], h, 0:1, :],
                        slot_l[way, j, picks[j][1], h, 0:1, :],
                    )
                    for j in range(2)
                ]
                peak = jnp.maximum(logs[0], logs[1])
                shares = [jnp.exp(one - peak) for one in logs]
                total = shares[0] + shares[1]
                made = 0.0
                for j in range(2):
                    both = jnp.where(
                        first_half,
                        slot[way, j, picks[j][0], h],
                        slot[way, j, picks[j][1], h],
                    )
                    made = made + both * (shares[j] / total)
                part[s, t, h * TILE : (h + 1) * TILE, :] = made
                part_l[s, h * tiles + t : h * tiles + t + 1, :] = peak + jnp.log(total)

    def delta(t, stage):
        ident = jnp.where(row_i == col_i, 1.0, 0.0)
        for h in range(heads):
            if stage == 0:
                lower = row_i >= col_i
                spread = cols[t, :, h : h + 1] - rows[t, h : h + 1, :]
                damping = jnp.where(lower, jnp.exp(jnp.where(lower, spread, 0.0)), 0.0)
                keys = kn[t, h]
                k_beta = keys * cols[t, :, 6 + h : 7 + h]
                inner = jnp.where(row_i > col_i, bdot(k_beta, keys, NT) * damping, 0.0)
                within[h] = jnp.where(lower, bdot(qn[t, h], keys, NT) * damping, 0.0)
                power[h] = inner
                inverse[h] = ident - inner
            elif stage < 3:
                value, made = power[h], inverse[h]
                for _ in range(3):
                    value = bdot(value, value)
                    made = bdot(made, ident + value)
                power[h] = value
                inverse[h] = made
            else:
                beta = cols[t, :, 6 + h : 7 + h]
                grown = cols[t, :, 2 + h : 3 + h]
                keys = kn[t, h]
                made = inverse[h]
                now = state[h]
                base = bdot(made, vn[t, h] * beta)
                mix = bdot(made, keys * beta * grown)
                fresh = base - bdot(mix, now)
                result = bdot(qn[t, h] * grown, now) + bdot(within[h], fresh)
                tail = keys * cols[t, :, 4 + h : 5 + h]
                state[h] = now * grown[TILE - 1 : TILE, :] + bdot(tail, fresh, TN)
                spread = jnp.mean(result * result, axis=1, keepdims=True)
                normed[t, h] = result * lax.rsqrt(spread + EPS) * gain[...]

    for which in range(2):
        kv_copy(which).start()
    for way in range(2):
        q_copy(way, 1, tiles).wait_recv()
        q_copy(way, 2, tiles).start()
        sm_copy(way, (1, far + 1)[way], 1).start()
    for c in range(tiles):
        forward(1, c)
        if c == 0:
            for index, ref in ((3, wq_h), (4, wk_h), (5, wv_h)):
                load_w(index, ref).wait()
            for copy in small[2:]:
                copy.wait()
        project_tokens(c)
    for which in range(2):
        kv_copy(which).wait_recv()

    def hop(k, carry):
        parity = lax.rem(k, 2)
        before = 1 - parity
        forward(k, tiles)
        for way in range(2):
            sm_copy(way, (k, far + k)[way], parity).start()
        for way in range(2):
            sm_copy(way, (k - 1, far + k - 1)[way], before).wait()
        for way in range(2):
            held[way] = qall[(k - 1, far + k - 1)[way]]
        for c in range(tiles):
            forward(k, c)
            for way in range(2):
                attend(way, before, c // 2, c % 2)
        for way in range(2):
            assemble((k - 1, far + k - 1)[way], way, before)
        return carry

    lax.fori_loop(2, near + 1, hop, 0)

    def whole(s, way, parity):
        held[way] = qall[s]
        for c in range(tiles):
            attend(way, parity, c // 2, c % 2)
        assemble(s, way, parity)

    def r_begin(way, s):
        ref, ref_l = ((ret1, ret1_l), (ret2, ret2_l))[way]
        ref_l[0] = part_l[s]
        for t in range(tiles):
            ref[0, t] = part[s, t].astype(jnp.bfloat16)
        for c in (tiles,) + tuple(range(tiles)):
            r_copy(way, 0, c).start()

    last = near % 2
    for way in range(2):
        sm_copy(way, (near, far + near)[way], last).wait()
    whole(far + near, 1, last)
    r_begin(1, far + near)
    q_copy(0, far, tiles).wait_recv()
    sm_copy(0, far, 1 - last).start()
    sm_copy(1, 0, 1 - last).start()
    for c in range(tiles):
        q_copy(0, far, c).wait_recv()
    sm_copy(0, far, 1 - last).wait()
    whole(far, 0, 1 - last)
    r_begin(0, far)
    whole(near, 0, last)
    sm_copy(1, 0, 1 - last).wait()
    whole(0, 1, 1 - last)

    def meet_logs(way, i, s):
        ref_l = (ret1_l, ret2_l)[way]
        r_copy(way, i - 1, tiles).wait_recv()
        theirs, mine = ref_l[i], part_l[s]
        peak = jnp.maximum(theirs, mine)
        shares = jnp.exp(theirs - peak), jnp.exp(mine - peak)
        total = shares[0] + shares[1]
        fac[way, 0] = shares[0] / total
        fac[way, 1] = shares[1] / total
        ref_l[i] = peak + jnp.log(total)

    def meet(way, i, s, t):
        ref = (ret1, ret2)[way]
        r_copy(way, i - 1, t).wait_recv()
        for h in range(heads):
            span = slice(h * TILE, (h + 1) * TILE)
            line = slice(h * tiles + t, h * tiles + t + 1)
            made = ref[i, t, span, :].astype(jnp.float32) * fac[way, 0, line, :]
            made = made + part[s, t, span, :] * fac[way, 1, line, :]
            ref[i, t, span, :] = made.astype(jnp.bfloat16)

    def back(i, carry):
        pair = far - i, far + near - i
        for way in range(2):
            meet_logs(way, i, pair[way])
        for c in range(tiles):
            for way in range(2):
                meet(way, i, pair[way], c)
            for way in range(2):
                if c == 0:
                    r_copy(way, i, tiles).start()
                r_copy(way, i, c).start()

            @pl.when(i <= tiles)
            def _():
                delta(i - 1, c)

        return carry

    lax.fori_loop(1, near, back, 0)
    meet_logs(0, near, far - near)
    for c in range(tiles):
        meet(0, near, far - near, c)
        if c == 0:
            r_copy(0, near, tiles).start()
        else:
            r_copy(0, near, c - 1).start()
    r_copy(1, near - 1, tiles).wait_recv()
    r_copy(0, near, tiles - 1).start()

    r_copy(0, far - 1, tiles).wait_recv()
    logs = part_l[0], ret1_l[far], ret2_l[near]
    peak = jnp.maximum(jnp.maximum(logs[0], logs[1]), logs[2])
    shares = [jnp.exp(one - peak) for one in logs]
    total = shares[0] + shares[1] + shares[2]
    shares = [one / total for one in shares]
    for t in range(tiles):
        r_copy(1, near - 1, t).wait_recv()
        r_copy(0, far - 1, t).wait_recv()
        for h in range(heads):
            span = slice(h * TILE, (h + 1) * TILE)
            line = slice(h * tiles + t, h * tiles + t + 1)
            made = part[0, t, span, :] * shares[0][line, :]
            made = made + ret1[far, t, span, :].astype(jnp.float32) * shares[1][line, :]
            made = made + ret2[near, t, span, :].astype(jnp.float32) * shares[2][line, :]
            made = jnp.transpose(made * rgate[t, h : h + 1, :])
            out[t * TILE : (t + 1) * TILE, span] = (normed[t, h] + made).astype(out.dtype)

    for which in range(2):
        kv_copy(which).wait_send()
    for way in range(2):
        hops = (far, near)[way]

        def drain(i, carry, way=way):
            for c in range(tiles + 1):
                q_copy(way, i + 1, c).wait_send()
                r_copy(way, i, c).wait_send()
            return carry

        lax.fori_loop(0, hops, drain, 0)


def per_device(
    tokens,
    owners,
    entries,
    store,
    mixer_query_weight,
    mixer_key_weight,
    mixer_value_weight,
    strength_weight,
    decay_weight,
    head_decay_rate,
    extra_forgetting_exponent,
    output_norm_gain,
    retrieval_query_weight,
    passage_key_weight,
    passage_value_weight,
    retrieval_gate_weight,
):
    heads = head_decay_rate.shape[0]
    length, model = tokens.shape
    width = mixer_query_weight.shape[1]
    blocks = owners.shape[0]
    passages, passage_rows = store.shape[:2]
    tiles = length // TILE
    chips = lax.axis_size("st") // 2
    far = chips // 2
    near = chips - 1 - far
    flat_store = store.reshape(passages * passage_rows, model)
    forget = extra_forgetting_exponent.reshape(tiles, TILE, heads).transpose(0, 2, 1)
    any_spec = pl.BlockSpec(memory_space=pl.ANY)
    vmem_spec = pl.BlockSpec(memory_space=pltpu.VMEM)
    f32, bf16 = jnp.float32, jnp.bfloat16
    square = (TILE, TILE)
    return pl.pallas_call(
        functools.partial(kernel, chips),
        out_shape=jax.ShapeDtypeStruct((length, width), bf16),
        in_specs=[any_spec] * 16,
        out_specs=vmem_spec,
        scratch_shapes=[
            pltpu.SMEM((owners.shape[1], blocks), jnp.int32),
            pltpu.SMEM((owners.shape[1], blocks), jnp.int32),
            pltpu.VMEM((heads, model), bf16),
            pltpu.VMEM((heads, model), bf16),
            pltpu.VMEM((heads, model), bf16),
            pltpu.VMEM((tiles, heads, TILE), f32),
            pltpu.VMEM((1, heads), f32),
            pltpu.VMEM((1, TILE), f32),
            pltpu.VMEM((length, model), bf16),
            pltpu.VMEM((passages * passage_rows, model), bf16),
            pltpu.VMEM((6, model, width), bf16),
            pltpu.VMEM((chips, blocks, BLOCK, width), bf16),
            pltpu.VMEM((chips, 8, TILE), jnp.int32),
            pltpu.SMEM((2, 2, 8, TILE), jnp.int32),
            pltpu.VMEM((2, blocks, BLOCK, width), bf16),
            pltpu.VMEM((2, 2, passages, passage_rows, width), bf16),
            pltpu.VMEM((2, 2, 3, heads) + square, f32),
            pltpu.VMEM((2, 2, 3, heads, 8, TILE), f32),
            pltpu.VMEM((chips, tiles, width, TILE), f32),
            pltpu.VMEM((chips, heads * tiles, TILE), f32),
            pltpu.VMEM((far + 1, tiles, width, TILE), bf16),
            pltpu.VMEM((far + 1, heads * tiles, TILE), f32),
            pltpu.VMEM((near + 1, tiles, width, TILE), bf16),
            pltpu.VMEM((near + 1, heads * tiles, TILE), f32),
            pltpu.VMEM((2, 2, heads * tiles, TILE), f32),
            pltpu.VMEM((tiles, heads) + square, f32),
            pltpu.VMEM((tiles, heads) + square, f32),
            pltpu.VMEM((tiles, heads) + square, f32),
            pltpu.VMEM((tiles, 8, TILE), f32),
            pltpu.VMEM((tiles, TILE, 8), f32),
            pltpu.VMEM((tiles, heads, TILE), f32),
            pltpu.VMEM((heads,) + square, f32),
            pltpu.VMEM((heads,) + square, f32),
            pltpu.VMEM((heads,) + square, f32),
            pltpu.VMEM((heads,) + square, f32),
            pltpu.VMEM((tiles, heads) + square, f32),
            pltpu.SemaphoreType.DMA((6 + 2 * tiles,)),
            pltpu.SemaphoreType.DMA((2, far, tiles + 1)),
            pltpu.SemaphoreType.DMA((2, far, tiles + 1)),
            pltpu.SemaphoreType.DMA((2, far, tiles + 1)),
            pltpu.SemaphoreType.DMA((2, far, tiles + 1)),
            pltpu.SemaphoreType.DMA((2,)),
            pltpu.SemaphoreType.DMA((2,)),
            pltpu.SemaphoreType.DMA((2, 2)),
            pltpu.SemaphoreType.DMA((8,)),
        ],
        compiler_params=pltpu.CompilerParams(
            collective_id=0, has_side_effects=True, vmem_limit_bytes=60 * 1024 * 1024
        ),
    )(
        tokens,
        flat_store,
        retrieval_query_weight,
        passage_key_weight,
        passage_value_weight,
        mixer_query_weight,
        mixer_key_weight,
        mixer_value_weight,
        owners.T,
        entries.T,
        strength_weight.T,
        decay_weight.T,
        retrieval_gate_weight.T,
        forget,
        head_decay_rate[None, :],
        output_norm_gain[None, :],
    )


def solution(mesh):
    return jax.shard_map(
        per_device,
        mesh=mesh,
        in_specs=(
            P(("grp", "st"), None),
            P(("grp", "st"), None),
            P(("grp", "st"), None),
            P(("grp", "st"), None, None),
            P(None, "tp"),
            P(None, "tp"),
            P(None, "tp"),
            P(None, "tp"),
            P(None, "tp"),
            P("tp"),
            P(("grp", "st"), "tp"),
            P(),
            P(None, "tp"),
            P(None, "tp"),
            P(None, "tp"),
            P(None, "tp"),
        ),
        out_specs=P(("grp", "st"), "tp"),
        check_vma=False,
    )
```

```python
import functools

import jax
import jax.numpy as jnp
from jax import lax
from jax.experimental import pallas as pl
from jax.experimental.pallas import tpu as pltpu
from jax.sharding import PartitionSpec as P

MESH = pl.DeviceIdType.MESH
EPS = 1e-06
NEVER = -1e30
BLOCK = 64
TILE = 128
NN = (((1,), (0,)), ((), ()))
NT = (((1,), (1,)), ((), ()))
TN = (((0,), (0,)), ((), ()))


def dot(left, right, dims=NN):
    return lax.dot_general(left, right, dims, preferred_element_type=jnp.float32)


def bdot(left, right, dims=NN):
    return dot(left.astype(jnp.bfloat16), right.astype(jnp.bfloat16), dims)


def rounded(array):
    return array.astype(jnp.bfloat16).astype(jnp.float32)


def kernel(
    chips,
    tok_h,
    store_h,
    wrq_h,
    wpk_h,
    wpv_h,
    wq_h,
    wk_h,
    wv_h,
    owners_h,
    entries_h,
    strength_h,
    decay_h,
    gate_h,
    forget_h,
    rate_h,
    gain_h,
    out,
    owners,
    entries,
    strength,
    decay,
    gate,
    forget,
    rate,
    gain,
    tok,
    store,
    wts,
    qall,
    meta,
    smeta,
    held,
    kv,
    slot,
    slot_l,
    part,
    part_l,
    ret1,
    ret1_l,
    ret2,
    ret2_l,
    fac,
    qn,
    kn,
    vn,
    rows,
    cols,
    rgate,
    power,
    inverse,
    within,
    state,
    normed,
    load_sem,
    q_send,
    q_recv,
    r_send,
    r_recv,
    kv_send,
    kv_recv,
    sm_sem,
    in_sem,
):
    far = chips // 2
    near = chips - 1 - far
    me = lax.axis_index("st")
    core = lax.rem(me, 2)
    chip = lax.div(me, 2)
    sign = 1 - 2 * core
    ahead = lax.rem(chip + sign + chips, chips) * 2 + core
    behind = lax.rem(chip - sign + chips, chips) * 2 + core
    peer = me + sign
    tiles = tok.shape[0] // TILE
    heads = slot.shape[3]
    chunks = 2 * heads
    some = qall.shape[2] // 2
    few = tiles // 2
    scale = TILE ** (-0.5)
    column = (me, peer)
    members = 2 * chips

    tok_rows = tok.shape[0] // tiles
    store_rows = store.shape[0] // tiles

    def load_w(index, ref):
        return pltpu.make_async_copy(ref, wts.at[index], load_sem.at[index])

    def load_tok(t):
        span = pl.ds(t * tok_rows, tok_rows)
        return pltpu.make_async_copy(tok_h.at[span], tok.at[span], load_sem.at[6 + t])

    def load_store(t):
        span = pl.ds(t * store_rows, store_rows)
        return pltpu.make_async_copy(
            store_h.at[span], store.at[span], load_sem.at[6 + tiles + t]
        )

    small = [
        pltpu.make_async_copy(src, dst, in_sem.at[index])
        for index, (src, dst) in enumerate(
            (
                (owners_h, owners),
                (entries_h, entries),
                (strength_h, strength),
                (decay_h, decay),
                (gate_h, gate),
                (forget_h, forget),
                (rate_h, rate),
                (gain_h, gain),
            )
        )
    ]
    for copy in small[:2]:
        copy.start()
    load_w(0, wrq_h).start()
    for t in range(tiles // 2):
        load_tok(t).start()
    barrier = pltpu.get_barrier_semaphore()
    for other in (ahead, behind, peer):
        pl.semaphore_signal(barrier, inc=1, device_id={"st": other}, device_id_type=MESH)

    lane = lax.broadcasted_iota(jnp.int32, (1, TILE), 1)
    count = jnp.zeros((1, TILE), jnp.int32)
    picks = [jnp.zeros((1, TILE), jnp.int32) for _ in range(4)]
    ranks = []
    for copy in small[:2]:
        copy.wait()
    for b in range(8):
        hit = jnp.zeros((1, TILE), jnp.int32)
        entry = jnp.zeros((1, TILE), jnp.int32)
        for i in range(owners.shape[0]):
            same = lane == owners[i, b]
            hit = jnp.where(same, 1, hit)
            entry = jnp.where(same, entries[i, b], entry)
        ranks.append(jnp.where(hit > 0, jnp.minimum(count, 2), 2))
        for r in range(2):
            chosen = (hit > 0) & (count == r)
            picks[2 * r] = jnp.where(chosen, b, picks[2 * r])
            picks[2 * r + 1] = jnp.where(chosen, entry, picks[2 * r + 1])
        count = count + hit
    for b in range(8):
        row = ranks[b]
        if b < 4:
            row = jnp.where(lane < members, row, pltpu.roll(picks[b], members, 1))
        meta[0, b : b + 1, :] = row

    def q_copy(way, k, c):
        if way == 0:
            source, target, device = k - 1, k, ahead
        else:
            source, target, device = jnp.where(k == 1, 0, far + k - 1), far + k, behind
        if c == chunks:
            src, dst = meta.at[source], meta.at[target]
        else:
            span = pl.ds(c % 2 * some, some)
            src, dst = qall.at[source, c // 2, span], qall.at[target, c // 2, span]
        return pltpu.make_async_remote_copy(
            src_ref=src,
            dst_ref=dst,
            send_sem=q_send.at[way, k - 1, c],
            recv_sem=q_recv.at[way, k - 1, c],
            device_id={"st": device},
            device_id_type=MESH,
        )

    def r_copy(way, i, c):
        ref, ref_l = ((ret1, ret1_l), (ret2, ret2_l))[way]
        if c >= chunks:
            src, dst = ref_l.at[i, c - chunks], ref_l.at[i + 1, c - chunks]
        else:
            span = pl.ds(c % 2 * few, few)
            src, dst = ref.at[i, c // 2, span], ref.at[i + 1, c // 2, span]
        return pltpu.make_async_remote_copy(
            src_ref=src,
            dst_ref=dst,
            send_sem=r_send.at[way, i, c],
            recv_sem=r_recv.at[way, i, c],
            device_id={"st": (behind, ahead)[way]},
            device_id_type=MESH,
        )

    def kv_copy(which):
        return pltpu.make_async_remote_copy(
            src_ref=kv.at[0, which],
            dst_ref=kv.at[1, which],
            send_sem=kv_send.at[which],
            recv_sem=kv_recv.at[which],
            device_id={"st": peer},
            device_id_type=MESH,
        )

    def sm_copy(way, index, slot_index):
        return pltpu.make_async_copy(
            meta.at[index], smeta.at[way, slot_index], sm_sem.at[way, slot_index]
        )

    load_w(0, wrq_h).wait()
    for t in range(tiles // 2, tiles):
        load_tok(t).start()
    pl.semaphore_wait(barrier, 3)
    for way in range(2):
        q_copy(way, 1, chunks).start()
    for t in range(tiles):
        load_tok(t).wait()
        own = dot(tok[t * tok_rows : (t + 1) * tok_rows, :], wts[0]).astype(jnp.bfloat16)
        for h in range(heads):
            one = own[:, h * TILE : (h + 1) * TILE]
            qall[0, h, 2 * t : 2 * t + 2] = one.reshape(2, BLOCK, TILE)
        if t == tiles // 2:
            for way in range(2):
                q_copy(way, 1, 0).start()

    slot[:, :, 2] = jnp.zeros(slot.shape[:2] + slot.shape[3:], slot.dtype)
    slot_l[:, :, 2] = jnp.full(slot_l.shape[:2] + slot_l.shape[3:], NEVER, jnp.float32)
    state[...] = jnp.zeros_like(state)
    for c in range(1, chunks):
        for way in range(2):
            q_copy(way, 1, c).start()
    load_w(1, wpk_h).start()
    load_w(2, wpv_h).start()
    for t in range(tiles):
        load_store(t).start()
    for copy in small[2:]:
        copy.start()

    group = kv.shape[2] // tiles

    def project_passages(t):
        load_store(t).wait()
        piece = store[pl.ds(t * store_rows, store_rows), :]
        for which in range(2):
            made = dot(piece, wts[1 + which]).astype(jnp.bfloat16)
            kv[0, which, pl.ds(t * group, group)] = made.reshape(group, BLOCK, made.shape[1])

    def forward(k, c):
        last_far = isinstance(k, int) and k >= far
        q_copy(0, k, c).wait_recv()
        if not last_far:
            q_copy(0, k + 1, c).start()
            q_copy(1, k, c).wait_recv()

            @pl.when(k < near)
            def _():
                q_copy(1, k + 1, c).start()

    row_i = lax.broadcasted_iota(jnp.int32, (TILE, TILE), 0)
    col_i = lax.broadcasted_iota(jnp.int32, (TILE, TILE), 1)
    first_half = lax.broadcasted_iota(jnp.int32, (1, TILE), 1) < BLOCK

    def project_tokens(t):
        rates = jnp.where(
            lax.broadcasted_iota(jnp.int32, (heads, TILE), 0) == 0, rate[0:1, 0:1], rate[0:1, 1:2]
        )
        piece = tok[t * tok_rows : (t + 1) * tok_rows, :]
        for index, ref in ((3, qn), (4, kn), (5, vn)):
            made = rounded(dot(piece, wts[index]))
            for h in range(heads):
                one = made[:, h * TILE : (h + 1) * TILE]
                if index < 5:
                    one = one * lax.rsqrt(jnp.sum(one * one, axis=1, keepdims=True) + EPS)
                if index == 3:
                    one = one * scale
                ref[t, h] = one
        small_w = jnp.concatenate(
            [strength[...], decay[...], gate[...], jnp.zeros((2, tok.shape[1]), tok.dtype)], axis=0
        )
        gates = jnp.transpose(dot(piece, small_w, NT))
        beta = jax.nn.sigmoid(gates[0:2, :])
        raw = gates[2:4, :]
        soft = jnp.maximum(raw, 0.0) + jnp.log1p(jnp.exp(-jnp.abs(raw)))
        cumul = -rates * soft + forget[t]
        spot = lax.broadcasted_iota(jnp.int32, cumul.shape, 1)
        shift = 1
        while shift < TILE:
            cumul = cumul + jnp.where(spot >= shift, pltpu.roll(cumul, shift, 1), 0.0)
            shift *= 2
        tail = jnp.exp(cumul[:, TILE - 1 : TILE] - cumul)
        lines = jnp.concatenate([cumul, jnp.exp(cumul), tail, beta], axis=0)
        rows[t] = lines
        cols[t] = jnp.transpose(lines)
        rgate[t] = jax.nn.sigmoid(gates[4:6, :])

    def attend(spot, way, parity, j, r, which):
        block = smeta[way, parity, 2 * r, column[j] + members]
        passage = smeta[way, parity, 2 * r + 1, column[j] + members]
        for h in which:
            span = slice(h * TILE, (h + 1) * TILE)
            query = held[spot, h, block]
            query = jnp.concatenate([query, query], axis=0)
            scores = dot(kv[j, 0, passage, :, span], query, NT) * scale
            peak = jnp.max(scores, axis=0, keepdims=True)
            expo = jnp.exp(scores - peak)
            total = jnp.sum(expo, axis=0, keepdims=True)
            weights = (expo / total).astype(jnp.bfloat16)
            slot[spot, j, r, h] = dot(kv[j, 1, passage, :, span], weights, TN)
            slot_l[spot, j, r, h] = jnp.broadcast_to(peak + jnp.log(total), (8, TILE))

    def assemble(s, spot, way, parity, which):
        for t in range(tiles):
            picks = [
                [smeta[way, parity, 2 * t + half, column[j]] for half in range(2)]
                for j in range(2)
            ]
            for h in which:
                logs = [
                    jnp.where(
                        first_half,
                        slot_l[spot, j, picks[j][0], h, 0:1, :],
                        slot_l[spot, j, picks[j][1], h, 0:1, :],
                    )
                    for j in range(2)
                ]
                peak = jnp.maximum(logs[0], logs[1])
                shares = [jnp.exp(one - peak) for one in logs]
                total = shares[0] + shares[1]
                made = 0.0
                for j in range(2):
                    both = jnp.where(
                        first_half,
                        slot[spot, j, picks[j][0], h],
                        slot[spot, j, picks[j][1], h],
                    )
                    made = made + both * (shares[j] / total)
                part[s, h, t] = made
                part_l[s, h, t : t + 1, :] = peak + jnp.log(total)

    def delta(t, stage):
        ident = jnp.where(row_i == col_i, 1.0, 0.0)
        for h in range(heads):
            if stage == 0:
                lower = row_i >= col_i
                spread = cols[t, :, h : h + 1] - rows[t, h : h + 1, :]
                damping = jnp.where(lower, jnp.exp(jnp.where(lower, spread, 0.0)), 0.0)
                keys = kn[t, h]
                k_beta = keys * cols[t, :, 6 + h : 7 + h]
                inner = jnp.where(row_i > col_i, bdot(k_beta, keys, NT) * damping, 0.0)
                within[h] = jnp.where(lower, bdot(qn[t, h], keys, NT) * damping, 0.0)
                power[h] = inner
                inverse[h] = ident - inner
            elif stage < 3:
                value, made = power[h], inverse[h]
                for _ in range(3):
                    value = bdot(value, value)
                    made = bdot(made, ident + value)
                power[h] = value
                inverse[h] = made
            else:
                beta = cols[t, :, 6 + h : 7 + h]
                grown = cols[t, :, 2 + h : 3 + h]
                keys = kn[t, h]
                made = inverse[h]
                now = state[h]
                base = bdot(made, vn[t, h] * beta)
                mix = bdot(made, keys * beta * grown)
                fresh = base - bdot(mix, now)
                result = bdot(qn[t, h] * grown, now) + bdot(within[h], fresh)
                tail = keys * cols[t, :, 4 + h : 5 + h]
                state[h] = now * grown[TILE - 1 : TILE, :] + bdot(tail, fresh, TN)
                spread = jnp.mean(result * result, axis=1, keepdims=True)
                normed[t, h] = result * lax.rsqrt(spread + EPS) * gain[...]

    every = tuple(range(heads))
    forward(1, chunks)
    for c in range(chunks):
        forward(1, c)
        if c == 0:
            load_w(1, wpk_h).wait()
            load_w(2, wpv_h).wait()
        project_passages(c)
    for index, ref in ((3, wq_h), (4, wk_h), (5, wv_h)):
        load_w(index, ref).start()
    for which in range(2):
        kv_copy(which).start()
    forward(2, chunks)
    for way in range(2):
        sm_copy(way, (2, far + 2)[way], 0).start()
    for c in range(chunks):
        forward(2, c)
        if c == 0:
            for index, ref in ((3, wq_h), (4, wk_h), (5, wv_h)):
                load_w(index, ref).wait()
            for copy in small[2:]:
                copy.wait()
        project_tokens(c)
    for which in range(2):
        kv_copy(which).wait_recv()

    def enter(k, parity):
        forward(k, chunks)
        for way in range(2):
            sm_copy(way, (k, far + k)[way], parity).start()
        for way in range(2):
            sm_copy(way, (k - 1, far + k - 1)[way], 1 - parity).wait()
        for way in range(2):
            held[way] = qall[(k - 1, far + k - 1)[way]]

    def hop(k, carry):
        parity = lax.rem(k, 2)
        before = 1 - parity
        enter(k, parity)
        for c in range(4):
            forward(k, c)
            for way in range(2):
                attend(way, way, before, c // 2, c % 2, every)
        for way in range(2):
            assemble((k - 1, far + k - 1)[way], way, way, before, every)
        return carry

    lax.fori_loop(3, near, hop, 0)

    def whole(s, spot, way, parity, which):
        for h in which:
            held[spot, h] = qall[s, h]
        for c in range(4):
            attend(spot, way, parity, c // 2, c % 2, which)
        assemble(s, spot, way, parity, which)

    def r_begin(way, s, h):
        ref, ref_l = ((ret1, ret1_l), (ret2, ret2_l))[way]
        ref_l[0, h] = part_l[s, h]
        ref[0, h] = part[s, h].astype(jnp.bfloat16)
        for c in (chunks + h, 2 * h, 2 * h + 1):
            r_copy(way, 0, c).start()

    last = near % 2
    before = 1 - last
    enter(near, last)
    sm_copy(1, far + near, last).wait()
    for c in range(4):
        forward(near, c)
        for way in range(2):
            attend(way, way, before, c // 2, c % 2, every)
        if c % 2:
            whole(far + near, 2, 1, last, (c // 2,))
            r_begin(1, far + near, c // 2)
    q_copy(0, far, chunks).wait_recv()
    sm_copy(0, far, 2).start()
    sm_copy(1, far + 1, last).start()
    sm_copy(0, near, last).wait()
    sm_copy(0, far, 2).wait()
    for h in range(heads):
        q_copy(0, far, 2 * h).wait_recv()
        q_copy(0, far, 2 * h + 1).wait_recv()
        whole(far, 2, 0, 2, (h,))
        r_begin(0, far, h)
        if h == 0:
            for way in range(2):
                assemble((near - 1, far + near - 1)[way], way, way, before, every)
            sm_copy(1, 0, before).start()
            sm_copy(0, 1, before).start()
        whole(near, 0, 0, last, (h,))
    sm_copy(1, far + 1, last).wait()
    sm_copy(1, 0, before).wait()
    sm_copy(0, 1, before).wait()

    def meet_logs(way, i, s, h):
        ref_l = (ret1_l, ret2_l)[way]
        r_copy(way, i - 1, chunks + h).wait_recv()
        theirs, mine = ref_l[i, h], part_l[s, h]
        peak = jnp.maximum(theirs, mine)
        shares = jnp.exp(theirs - peak), jnp.exp(mine - peak)
        total = shares[0] + shares[1]
        fac[way, 0, h] = shares[0] / total
        fac[way, 1, h] = shares[1] / total
        ref_l[i, h] = peak + jnp.log(total)

    def meet(way, i, s, c):
        ref = (ret1, ret2)[way]
        h = c // 2
        r_copy(way, i - 1, c).wait_recv()
        for t in range(c % 2 * few, c % 2 * few + few):
            made = ref[i, h, t].astype(jnp.float32) * fac[way, 0, h, t : t + 1, :]
            made = made + part[s, h, t] * fac[way, 1, h, t : t + 1, :]
            ref[i, h, t] = made.astype(jnp.bfloat16)

    def back(i, carry):
        pair = far - i, far + near - i
        for c in range(chunks):
            if c % 2 == 0:
                for way in range(2):
                    meet_logs(way, i, pair[way], c // 2)
            for way in range(2):
                meet(way, i, pair[way], c)
            for way in range(2):
                if c % 2 == 0:
                    r_copy(way, i, chunks + c // 2).start()
                r_copy(way, i, c).start()

            @pl.when(i <= tiles)
            def _():
                delta(i - 1, c)

        @pl.when(i <= 3)
        def _():
            way = i % 2
            index = jnp.where(i == 1, far + 1, jnp.where(i == 2, 1, 0))
            whole(index, 0, way, jnp.where(i == 1, last, before), every)

        return carry

    lax.fori_loop(1, near, back, 0)
    for c in range(chunks):
        if c % 2 == 0:
            meet_logs(0, near, far - near, c // 2)
        meet(0, near, far - near, c)
        if c % 2:
            r_copy(0, near, chunks + c // 2).start()
            r_copy(0, near, c - 1).start()
            r_copy(0, near, c).start()

    for h in range(heads):
        span = slice(h * TILE, (h + 1) * TILE)
        r_copy(1, near - 1, chunks + h).wait_recv()
        r_copy(0, far - 1, chunks + h).wait_recv()
        logs = part_l[0, h], ret1_l[far, h], ret2_l[near, h]
        peak = jnp.maximum(jnp.maximum(logs[0], logs[1]), logs[2])
        shares = [jnp.exp(one - peak) for one in logs]
        total = shares[0] + shares[1] + shares[2]
        shares = [one / total for one in shares]
        for t in range(tiles):
            if t % few == 0:
                r_copy(1, near - 1, 2 * h + t // few).wait_recv()
                r_copy(0, far - 1, 2 * h + t // few).wait_recv()
            made = part[0, h, t] * shares[0][t : t + 1, :]
            made = made + ret1[far, h, t].astype(jnp.float32) * shares[1][t : t + 1, :]
            made = made + ret2[near, h, t].astype(jnp.float32) * shares[2][t : t + 1, :]
            made = jnp.transpose(made * rgate[t, h : h + 1, :])
            out[t * TILE : (t + 1) * TILE, span] = (normed[t, h] + made).astype(out.dtype)

    for which in range(2):
        kv_copy(which).wait_send()
    for way in range(2):
        hops = (far, near)[way]

        def drain(i, carry, way=way):
            for c in range(chunks + 1):
                q_copy(way, i + 1, c).wait_send()
            for c in range(chunks + heads):
                r_copy(way, i, c).wait_send()
            return carry

        lax.fori_loop(0, hops, drain, 0)


def per_device(
    tokens,
    owners,
    entries,
    store,
    mixer_query_weight,
    mixer_key_weight,
    mixer_value_weight,
    strength_weight,
    decay_weight,
    head_decay_rate,
    extra_forgetting_exponent,
    output_norm_gain,
    retrieval_query_weight,
    passage_key_weight,
    passage_value_weight,
    retrieval_gate_weight,
):
    heads = head_decay_rate.shape[0]
    length, model = tokens.shape
    width = mixer_query_weight.shape[1]
    blocks = owners.shape[0]
    passages, passage_rows = store.shape[:2]
    tiles = length // TILE
    chips = lax.axis_size("st") // 2
    far = chips // 2
    near = chips - 1 - far
    flat_store = store.reshape(passages * passage_rows, model)
    forget = extra_forgetting_exponent.reshape(tiles, TILE, heads).transpose(0, 2, 1)
    any_spec = pl.BlockSpec(memory_space=pl.ANY)
    vmem_spec = pl.BlockSpec(memory_space=pltpu.VMEM)
    f32, bf16 = jnp.float32, jnp.bfloat16
    square = (TILE, TILE)
    return pl.pallas_call(
        functools.partial(kernel, chips),
        out_shape=jax.ShapeDtypeStruct((length, width), bf16),
        in_specs=[any_spec] * 16,
        out_specs=vmem_spec,
        scratch_shapes=[
            pltpu.SMEM((owners.shape[1], blocks), jnp.int32),
            pltpu.SMEM((owners.shape[1], blocks), jnp.int32),
            pltpu.VMEM((heads, model), bf16),
            pltpu.VMEM((heads, model), bf16),
            pltpu.VMEM((heads, model), bf16),
            pltpu.VMEM((tiles, heads, TILE), f32),
            pltpu.VMEM((1, heads), f32),
            pltpu.VMEM((1, TILE), f32),
            pltpu.VMEM((length, model), bf16),
            pltpu.VMEM((passages * passage_rows, model), bf16),
            pltpu.VMEM((6, model, width), bf16),
            pltpu.VMEM((chips, heads, blocks, BLOCK, TILE), bf16),
            pltpu.VMEM((chips, 8, TILE), jnp.int32),
            pltpu.SMEM((2, 3, 8, TILE), jnp.int32),
            pltpu.VMEM((3, heads, blocks, BLOCK, TILE), bf16),
            pltpu.VMEM((2, 2, passages, passage_rows, width), bf16),
            pltpu.VMEM((3, 2, 3, heads) + square, f32),
            pltpu.VMEM((3, 2, 3, heads, 8, TILE), f32),
            pltpu.VMEM((chips, heads, tiles) + square, f32),
            pltpu.VMEM((chips, heads, tiles, TILE), f32),
            pltpu.VMEM((far + 1, heads, tiles) + square, bf16),
            pltpu.VMEM((far + 1, heads, tiles, TILE), f32),
            pltpu.VMEM((near + 1, heads, tiles) + square, bf16),
            pltpu.VMEM((near + 1, heads, tiles, TILE), f32),
            pltpu.VMEM((2, 2, heads, tiles, TILE), f32),
            pltpu.VMEM((tiles, heads) + square, f32),
            pltpu.VMEM((tiles, heads) + square, f32),
            pltpu.VMEM((tiles, heads) + square, f32),
            pltpu.VMEM((tiles, 8, TILE), f32),
            pltpu.VMEM((tiles, TILE, 8), f32),
            pltpu.VMEM((tiles, heads, TILE), f32),
            pltpu.VMEM((heads,) + square, f32),
            pltpu.VMEM((heads,) + square, f32),
            pltpu.VMEM((heads,) + square, f32),
            pltpu.VMEM((heads,) + square, f32),
            pltpu.VMEM((tiles, heads) + square, f32),
            pltpu.SemaphoreType.DMA((6 + 2 * tiles,)),
            pltpu.SemaphoreType.DMA((2, far, 2 * heads + 1)),
            pltpu.SemaphoreType.DMA((2, far, 2 * heads + 1)),
            pltpu.SemaphoreType.DMA((2, far, 3 * heads)),
            pltpu.SemaphoreType.DMA((2, far, 3 * heads)),
            pltpu.SemaphoreType.DMA((2,)),
            pltpu.SemaphoreType.DMA((2,)),
            pltpu.SemaphoreType.DMA((2, 3)),
            pltpu.SemaphoreType.DMA((8,)),
        ],
        compiler_params=pltpu.CompilerParams(
            collective_id=0, has_side_effects=True, vmem_limit_bytes=60 * 1024 * 1024
        ),
    )(
        tokens,
        flat_store,
        retrieval_query_weight,
        passage_key_weight,
        passage_value_weight,
        mixer_query_weight,
        mixer_key_weight,
        mixer_value_weight,
        owners.T,
        entries.T,
        strength_weight.T,
        decay_weight.T,
        retrieval_gate_weight.T,
        forget,
        head_decay_rate[None, :],
        output_norm_gain[None, :],
    )


def solution(mesh):
    return jax.shard_map(
        per_device,
        mesh=mesh,
        in_specs=(
            P(("grp", "st"), None),
            P(("grp", "st"), None),
            P(("grp", "st"), None),
            P(("grp", "st"), None, None),
            P(None, "tp"),
            P(None, "tp"),
            P(None, "tp"),
            P(None, "tp"),
            P(None, "tp"),
            P("tp"),
            P(("grp", "st"), "tp"),
            P(),
            P(None, "tp"),
            P(None, "tp"),
            P(None, "tp"),
            P(None, "tp"),
        ),
        out_specs=P(("grp", "st"), "tp"),
        check_vma=False,
    )
```

```python
import functools

import jax
import jax.numpy as jnp
from jax import lax
from jax.experimental import pallas as pl
from jax.experimental.pallas import tpu as pltpu
from jax.sharding import PartitionSpec as P

MESH = pl.DeviceIdType.MESH
EPS = 1e-06
NEVER = -1e30
BLOCK = 64
TILE = 128
NN = (((1,), (0,)), ((), ()))
NT = (((1,), (1,)), ((), ()))
TN = (((0,), (0,)), ((), ()))


def dot(left, right, dims=NN):
    return lax.dot_general(left, right, dims, preferred_element_type=jnp.float32)


def bdot(left, right, dims=NN):
    return dot(left.astype(jnp.bfloat16), right.astype(jnp.bfloat16), dims)


def rounded(array):
    return array.astype(jnp.bfloat16).astype(jnp.float32)


def kernel(
    chips,
    tok_h,
    store_h,
    wrq_h,
    wpk_h,
    wpv_h,
    wq_h,
    wk_h,
    wv_h,
    owners_h,
    entries_h,
    strength_h,
    decay_h,
    gate_h,
    forget_h,
    rate_h,
    gain_h,
    out,
    owners,
    entries,
    strength,
    decay,
    gate,
    forget,
    rate,
    gain,
    tok,
    store,
    wts,
    qall,
    meta,
    smeta,
    held,
    kv,
    slot,
    slot_l,
    part,
    part_l,
    ret1,
    ret1_l,
    ret2,
    ret2_l,
    fac,
    qn,
    kn,
    vn,
    rows,
    cols,
    rgate,
    power,
    inverse,
    within,
    state,
    normed,
    load_sem,
    q_send,
    q_recv,
    r_send,
    r_recv,
    kv_send,
    kv_recv,
    sm_sem,
    in_sem,
):
    far = chips // 2
    near = chips - 1 - far
    me = lax.axis_index("st")
    core = lax.rem(me, 2)
    chip = lax.div(me, 2)
    sign = 1 - 2 * core
    ahead = lax.rem(chip + sign + chips, chips) * 2 + core
    behind = lax.rem(chip - sign + chips, chips) * 2 + core
    peer = me + sign
    tiles = tok.shape[0] // TILE
    heads = slot.shape[3]
    chunks = 2 * heads
    some = qall.shape[2] // 2
    few = tiles // 2
    scale = TILE ** (-0.5)
    column = (me, peer)
    members = 2 * chips

    tok_rows = tok.shape[0] // tiles
    store_rows = store.shape[0] // tiles

    def load_w(index, ref):
        return pltpu.make_async_copy(ref, wts.at[index], load_sem.at[index])

    def load_tok(t):
        span = pl.ds(t * tok_rows, tok_rows)
        return pltpu.make_async_copy(tok_h.at[span], tok.at[span], load_sem.at[6 + t])

    def load_store(t):
        span = pl.ds(t * store_rows, store_rows)
        return pltpu.make_async_copy(
            store_h.at[span], store.at[span], load_sem.at[6 + tiles + t]
        )

    small = [
        pltpu.make_async_copy(src, dst, in_sem.at[index])
        for index, (src, dst) in enumerate(
            (
                (owners_h, owners),
                (entries_h, entries),
                (strength_h, strength),
                (decay_h, decay),
                (gate_h, gate),
                (forget_h, forget),
                (rate_h, rate),
                (gain_h, gain),
            )
        )
    ]
    for copy in small[:2]:
        copy.start()
    load_w(0, wrq_h).start()
    for t in range(tiles // 2):
        load_tok(t).start()
    barrier = pltpu.get_barrier_semaphore()
    for other in (ahead, behind, peer):
        pl.semaphore_signal(barrier, inc=1, device_id={"st": other}, device_id_type=MESH)

    lane = lax.broadcasted_iota(jnp.int32, (1, TILE), 1)
    count = jnp.zeros((1, TILE), jnp.int32)
    picks = [jnp.zeros((1, TILE), jnp.int32) for _ in range(4)]
    ranks = []
    for copy in small[:2]:
        copy.wait()
    for b in range(8):
        hit = jnp.zeros((1, TILE), jnp.int32)
        entry = jnp.zeros((1, TILE), jnp.int32)
        for i in range(owners.shape[0]):
            same = lane == owners[i, b]
            hit = jnp.where(same, 1, hit)
            entry = jnp.where(same, entries[i, b], entry)
        ranks.append(jnp.where(hit > 0, jnp.minimum(count, 2), 2))
        for r in range(2):
            chosen = (hit > 0) & (count == r)
            picks[2 * r] = jnp.where(chosen, b, picks[2 * r])
            picks[2 * r + 1] = jnp.where(chosen, entry, picks[2 * r + 1])
        count = count + hit
    for b in range(8):
        row = ranks[b]
        if b < 4:
            row = jnp.where(lane < members, row, pltpu.roll(picks[b], members, 1))
        meta[0, b : b + 1, :] = row

    def q_copy(way, k, c):
        if way == 0:
            source, target, device = k - 1, k, ahead
        else:
            source, target, device = jnp.where(k == 1, 0, far + k - 1), far + k, behind
        if c == chunks:
            src, dst = meta.at[source], meta.at[target]
        else:
            span = pl.ds(c % 2 * some, some)
            src, dst = qall.at[source, c // 2, span], qall.at[target, c // 2, span]
        return pltpu.make_async_remote_copy(
            src_ref=src,
            dst_ref=dst,
            send_sem=q_send.at[way, k - 1, c],
            recv_sem=q_recv.at[way, k - 1, c],
            device_id={"st": device},
            device_id_type=MESH,
        )

    def r_copy(way, i, c):
        ref, ref_l = ((ret1, ret1_l), (ret2, ret2_l))[way]
        if c >= chunks:
            src, dst = ref_l.at[i, c - chunks], ref_l.at[i + 1, c - chunks]
        else:
            span = pl.ds(c % 2 * few, few)
            src, dst = ref.at[i, c // 2, span], ref.at[i + 1, c // 2, span]
        return pltpu.make_async_remote_copy(
            src_ref=src,
            dst_ref=dst,
            send_sem=r_send.at[way, i, c],
            recv_sem=r_recv.at[way, i, c],
            device_id={"st": (behind, ahead)[way]},
            device_id_type=MESH,
        )

    def kv_copy(which):
        return pltpu.make_async_remote_copy(
            src_ref=kv.at[0, which],
            dst_ref=kv.at[1, which],
            send_sem=kv_send.at[which],
            recv_sem=kv_recv.at[which],
            device_id={"st": peer},
            device_id_type=MESH,
        )

    def sm_copy(way, index, slot_index):
        return pltpu.make_async_copy(
            meta.at[index], smeta.at[way, slot_index], sm_sem.at[way, slot_index]
        )

    load_w(0, wrq_h).wait()
    for t in range(tiles // 2, tiles):
        load_tok(t).start()
    pl.semaphore_wait(barrier, 3)
    for way in range(2):
        q_copy(way, 1, chunks).start()
    for t in range(tiles):
        load_tok(t).wait()
        own = dot(tok[t * tok_rows : (t + 1) * tok_rows, :], wts[0]).astype(jnp.bfloat16)
        for h in range(heads):
            one = own[:, h * TILE : (h + 1) * TILE]
            qall[0, h, 2 * t : 2 * t + 2] = one.reshape(2, BLOCK, TILE)
        if t == tiles // 2:
            for way in range(2):
                q_copy(way, 1, 0).start()

    slot[:, :, 2] = jnp.zeros(slot.shape[:2] + slot.shape[3:], slot.dtype)
    slot_l[:, :, 2] = jnp.full(slot_l.shape[:2] + slot_l.shape[3:], NEVER, jnp.float32)
    state[...] = jnp.zeros_like(state)
    for c in range(1, chunks):
        for way in range(2):
            q_copy(way, 1, c).start()
    load_w(1, wpk_h).start()
    load_w(2, wpv_h).start()
    for t in range(tiles):
        load_store(t).start()
    for copy in small[2:]:
        copy.start()

    group = kv.shape[2] // tiles

    def project_passages(t):
        load_store(t).wait()
        piece = store[pl.ds(t * store_rows, store_rows), :]
        for which in range(2):
            made = dot(piece, wts[1 + which]).astype(jnp.bfloat16)
            kv[0, which, pl.ds(t * group, group)] = made.reshape(group, BLOCK, made.shape[1])

    def forward(k, c):
        last_far = isinstance(k, int) and k >= far
        q_copy(0, k, c).wait_recv()
        if not last_far:
            q_copy(0, k + 1, c).start()
            q_copy(1, k, c).wait_recv()

            @pl.when(k < near)
            def _():
                q_copy(1, k + 1, c).start()

    row_i = lax.broadcasted_iota(jnp.int32, (TILE, TILE), 0)
    col_i = lax.broadcasted_iota(jnp.int32, (TILE, TILE), 1)
    first_half = lax.broadcasted_iota(jnp.int32, (1, TILE), 1) < BLOCK

    def project_tokens(t):
        rates = jnp.where(
            lax.broadcasted_iota(jnp.int32, (heads, TILE), 0) == 0, rate[0:1, 0:1], rate[0:1, 1:2]
        )
        piece = tok[t * tok_rows : (t + 1) * tok_rows, :]
        for index, ref in ((3, qn), (4, kn), (5, vn)):
            made = rounded(dot(piece, wts[index]))
            for h in range(heads):
                one = made[:, h * TILE : (h + 1) * TILE]
                if index < 5:
                    one = one * lax.rsqrt(jnp.sum(one * one, axis=1, keepdims=True) + EPS)
                if index == 3:
                    one = one * scale
                ref[t, h] = one
        small_w = jnp.concatenate(
            [strength[...], decay[...], gate[...], jnp.zeros((2, tok.shape[1]), tok.dtype)], axis=0
        )
        gates = jnp.transpose(dot(piece, small_w, NT))
        beta = jax.nn.sigmoid(gates[0:2, :])
        raw = gates[2:4, :]
        soft = jnp.maximum(raw, 0.0) + jnp.log1p(jnp.exp(-jnp.abs(raw)))
        cumul = -rates * soft + forget[t]
        spot = lax.broadcasted_iota(jnp.int32, cumul.shape, 1)
        shift = 1
        while shift < TILE:
            cumul = cumul + jnp.where(spot >= shift, pltpu.roll(cumul, shift, 1), 0.0)
            shift *= 2
        tail = jnp.exp(cumul[:, TILE - 1 : TILE] - cumul)
        lines = jnp.concatenate([cumul, jnp.exp(cumul), tail, beta], axis=0)
        rows[t] = lines
        cols[t] = jnp.transpose(lines)
        rgate[t] = jax.nn.sigmoid(gates[4:6, :])

    def attend(spot, way, parity, j, r, which):
        block = smeta[way, parity, 2 * r, column[j] + members]
        passage = smeta[way, parity, 2 * r + 1, column[j] + members]
        for h in which:
            span = slice(h * TILE, (h + 1) * TILE)
            query = held[spot, h, block]
            query = jnp.concatenate([query, query], axis=0)
            scores = dot(kv[j, 0, passage, :, span], query, NT) * scale
            peak = jnp.max(scores, axis=0, keepdims=True)
            expo = jnp.exp(scores - peak)
            total = jnp.sum(expo, axis=0, keepdims=True)
            weights = (expo / total).astype(jnp.bfloat16)
            slot[spot, j, r, h] = dot(kv[j, 1, passage, :, span], weights, TN)
            slot_l[spot, j, r, h] = jnp.broadcast_to(peak + jnp.log(total), (8, TILE))

    def assemble(s, spot, way, parity, which):
        for t in range(tiles):
            picks = [
                [smeta[way, parity, 2 * t + half, column[j]] for half in range(2)]
                for j in range(2)
            ]
            for h in which:
                logs = [
                    jnp.where(
                        first_half,
                        slot_l[spot, j, picks[j][0], h, 0:1, :],
                        slot_l[spot, j, picks[j][1], h, 0:1, :],
                    )
                    for j in range(2)
                ]
                peak = jnp.maximum(logs[0], logs[1])
                shares = [jnp.exp(one - peak) for one in logs]
                total = shares[0] + shares[1]
                made = 0.0
                for j in range(2):
                    both = jnp.where(
                        first_half,
                        slot[spot, j, picks[j][0], h],
                        slot[spot, j, picks[j][1], h],
                    )
                    made = made + both * (shares[j] / total)
                part[s, h, t] = made
                part_l[s, h, t : t + 1, :] = peak + jnp.log(total)

    def delta(t, stage):
        ident = jnp.where(row_i == col_i, 1.0, 0.0)
        for h in range(heads):
            if stage == 0:
                lower = row_i >= col_i
                spread = cols[t, :, h : h + 1] - rows[t, h : h + 1, :]
                damping = jnp.where(lower, jnp.exp(jnp.where(lower, spread, 0.0)), 0.0)
                keys = kn[t, h]
                k_beta = keys * cols[t, :, 6 + h : 7 + h]
                inner = jnp.where(row_i > col_i, bdot(k_beta, keys, NT) * damping, 0.0)
                within[h] = jnp.where(lower, bdot(qn[t, h], keys, NT) * damping, 0.0)
                power[h] = inner
                inverse[h] = ident - inner
            elif stage < 3:
                value, made = power[h], inverse[h]
                for _ in range(3):
                    value = bdot(value, value)
                    made = bdot(made, ident + value)
                power[h] = value
                inverse[h] = made
            else:
                beta = cols[t, :, 6 + h : 7 + h]
                grown = cols[t, :, 2 + h : 3 + h]
                keys = kn[t, h]
                made = inverse[h]
                now = state[h]
                base = bdot(made, vn[t, h] * beta)
                mix = bdot(made, keys * beta * grown)
                fresh = base - bdot(mix, now)
                result = bdot(qn[t, h] * grown, now) + bdot(within[h], fresh)
                tail = keys * cols[t, :, 4 + h : 5 + h]
                state[h] = now * grown[TILE - 1 : TILE, :] + bdot(tail, fresh, TN)
                spread = jnp.mean(result * result, axis=1, keepdims=True)
                normed[t, h] = result * lax.rsqrt(spread + EPS) * gain[...]

    every = tuple(range(heads))
    forward(1, chunks)
    for c in range(chunks):
        forward(1, c)
        if c == 0:
            load_w(1, wpk_h).wait()
            load_w(2, wpv_h).wait()
        project_passages(c)
    for index, ref in ((3, wq_h), (4, wk_h), (5, wv_h)):
        load_w(index, ref).start()
    for which in range(2):
        kv_copy(which).start()
    forward(2, chunks)
    for way in range(2):
        sm_copy(way, (2, far + 2)[way], 0).start()
    for c in range(chunks):
        forward(2, c)
        if c == 0:
            for index, ref in ((3, wq_h), (4, wk_h), (5, wv_h)):
                load_w(index, ref).wait()
            for copy in small[2:]:
                copy.wait()
        project_tokens(c)
    for which in range(2):
        kv_copy(which).wait_recv()

    def enter(k, parity):
        forward(k, chunks)
        for way in range(2):
            sm_copy(way, (k, far + k)[way], parity).start()
        for way in range(2):
            sm_copy(way, (k - 1, far + k - 1)[way], 1 - parity).wait()
        for way in range(2):
            held[way] = qall[(k - 1, far + k - 1)[way]]

    def hop(k, carry):
        parity = lax.rem(k, 2)
        before = 1 - parity
        enter(k, parity)
        for c in range(4):
            forward(k, c)
            for way in range(2):
                attend(way, way, before, c // 2, c % 2, every)
        for way in range(2):
            assemble((k - 1, far + k - 1)[way], way, way, before, every)
        return carry

    lax.fori_loop(3, near, hop, 0)

    def whole(s, spot, way, parity, which):
        for h in which:
            held[spot, h] = qall[s, h]
        for c in range(4):
            attend(spot, way, parity, c // 2, c % 2, which)
        assemble(s, spot, way, parity, which)

    def r_begin(way, s, h):
        ref, ref_l = ((ret1, ret1_l), (ret2, ret2_l))[way]
        ref_l[0, h] = part_l[s, h]
        ref[0, h] = part[s, h].astype(jnp.bfloat16)
        for c in (chunks + h, 2 * h, 2 * h + 1):
            r_copy(way, 0, c).start()

    last = near % 2
    before = 1 - last
    enter(near, last)
    sm_copy(1, far + near, last).wait()
    for c in range(4):
        forward(near, c)
        for way in range(2):
            attend(way, way, before, c // 2, c % 2, every)
        if c % 2:
            whole(far + near, 2, 1, last, (c // 2,))
            r_begin(1, far + near, c // 2)
    q_copy(0, far, chunks).wait_recv()
    sm_copy(0, far, 2).start()
    sm_copy(1, far + 1, last).start()
    sm_copy(0, near, last).wait()
    sm_copy(0, far, 2).wait()
    for h in range(heads):
        q_copy(0, far, 2 * h).wait_recv()
        q_copy(0, far, 2 * h + 1).wait_recv()
        whole(far, 2, 0, 2, (h,))
        r_begin(0, far, h)
        if h == 0:
            for way in range(2):
                assemble((near - 1, far + near - 1)[way], way, way, before, every)
            sm_copy(1, 0, before).start()
            sm_copy(0, 1, before).start()
        whole(near, 0, 0, last, (h,))
    sm_copy(1, far + 1, last).wait()
    sm_copy(1, 0, before).wait()
    sm_copy(0, 1, before).wait()

    def meet_logs(way, i, s, h):
        ref_l = (ret1_l, ret2_l)[way]
        r_copy(way, i - 1, chunks + h).wait_recv()
        theirs, mine = ref_l[i, h], part_l[s, h]
        peak = jnp.maximum(theirs, mine)
        shares = jnp.exp(theirs - peak), jnp.exp(mine - peak)
        total = shares[0] + shares[1]
        fac[way, 0, h] = shares[0] / total
        fac[way, 1, h] = shares[1] / total
        ref_l[i, h] = peak + jnp.log(total)

    def meet(way, i, s, c):
        ref = (ret1, ret2)[way]
        h = c // 2
        r_copy(way, i - 1, c).wait_recv()
        for t in range(c % 2 * few, c % 2 * few + few):
            made = ref[i, h, t].astype(jnp.float32) * fac[way, 0, h, t : t + 1, :]
            made = made + part[s, h, t] * fac[way, 1, h, t : t + 1, :]
            ref[i, h, t] = made.astype(jnp.bfloat16)

    def back(i, carry):
        pair = far - i, far + near - i
        for c in range(chunks):
            if c % 2 == 0:
                for way in range(2):
                    meet_logs(way, i, pair[way], c // 2)
            for way in range(2):
                meet(way, i, pair[way], c)
            for way in range(2):
                if c % 2 == 0:
                    r_copy(way, i, chunks + c // 2).start()
                r_copy(way, i, c).start()

            @pl.when(i <= tiles)
            def _():
                delta(i - 1, c)

        @pl.when(i <= 3)
        def _():
            way = i % 2
            index = jnp.where(i == 1, far + 1, jnp.where(i == 2, 1, 0))
            whole(index, 0, way, jnp.where(i == 1, last, before), every)

        return carry

    lax.fori_loop(1, near, back, 0)
    for c in range(chunks):
        if c % 2 == 0:
            meet_logs(0, near, far - near, c // 2)
        meet(0, near, far - near, c)
        if c % 2:
            r_copy(0, near, chunks + c // 2).start()
            r_copy(0, near, c - 1).start()
            r_copy(0, near, c).start()

    for h in range(heads):
        span = slice(h * TILE, (h + 1) * TILE)
        r_copy(1, near - 1, chunks + h).wait_recv()
        r_copy(0, far - 1, chunks + h).wait_recv()
        logs = part_l[0, h], ret1_l[far, h], ret2_l[near, h]
        peak = jnp.maximum(jnp.maximum(logs[0], logs[1]), logs[2])
        shares = [jnp.exp(one - peak) for one in logs]
        total = shares[0] + shares[1] + shares[2]
        shares = [one / total for one in shares]
        for t in range(tiles):
            if t % few == 0:
                r_copy(1, near - 1, 2 * h + t // few).wait_recv()
                r_copy(0, far - 1, 2 * h + t // few).wait_recv()
            made = part[0, h, t] * shares[0][t : t + 1, :]
            made = made + ret1[far, h, t].astype(jnp.float32) * shares[1][t : t + 1, :]
            made = made + ret2[near, h, t].astype(jnp.float32) * shares[2][t : t + 1, :]
            made = jnp.transpose(made * rgate[t, h : h + 1, :])
            out[t * TILE : (t + 1) * TILE, span] = (normed[t, h] + made).astype(out.dtype)

    for which in range(2):
        kv_copy(which).wait_send()
    for way in range(2):
        hops = (far, near)[way]

        def drain(i, carry, way=way):
            for c in range(chunks + 1):
                q_copy(way, i + 1, c).wait_send()
            for c in range(chunks + heads):
                r_copy(way, i, c).wait_send()
            return carry

        lax.fori_loop(0, hops, drain, 0)


def per_device(
    tokens,
    owners,
    entries,
    store,
    mixer_query_weight,
    mixer_key_weight,
    mixer_value_weight,
    strength_weight,
    decay_weight,
    head_decay_rate,
    extra_forgetting_exponent,
    output_norm_gain,
    retrieval_query_weight,
    passage_key_weight,
    passage_value_weight,
    retrieval_gate_weight,
):
    heads = head_decay_rate.shape[0]
    length, model = tokens.shape
    width = mixer_query_weight.shape[1]
    blocks = owners.shape[0]
    passages, passage_rows = store.shape[:2]
    tiles = length // TILE
    chips = lax.axis_size("st") // 2
    far = chips // 2
    near = chips - 1 - far
    flat_store = store.reshape(passages * passage_rows, model)
    forget = extra_forgetting_exponent.reshape(tiles, TILE, heads).transpose(0, 2, 1)
    any_spec = pl.BlockSpec(memory_space=pl.ANY)
    vmem_spec = pl.BlockSpec(memory_space=pltpu.VMEM)
    f32, bf16 = jnp.float32, jnp.bfloat16
    square = (TILE, TILE)
    return pl.pallas_call(
        functools.partial(kernel, chips),
        out_shape=pltpu.VMEM((length, width), bf16),
        in_specs=[any_spec] * 16,
        out_specs=vmem_spec,
        scratch_shapes=[
            pltpu.SMEM((owners.shape[1], blocks), jnp.int32),
            pltpu.SMEM((owners.shape[1], blocks), jnp.int32),
            pltpu.VMEM((heads, model), bf16),
            pltpu.VMEM((heads, model), bf16),
            pltpu.VMEM((heads, model), bf16),
            pltpu.VMEM((tiles, heads, TILE), f32),
            pltpu.VMEM((1, heads), f32),
            pltpu.VMEM((1, TILE), f32),
            pltpu.VMEM((length, model), bf16),
            pltpu.VMEM((passages * passage_rows, model), bf16),
            pltpu.VMEM((6, model, width), bf16),
            pltpu.VMEM((chips, heads, blocks, BLOCK, TILE), bf16),
            pltpu.VMEM((chips, 8, TILE), jnp.int32),
            pltpu.SMEM((2, 3, 8, TILE), jnp.int32),
            pltpu.VMEM((3, heads, blocks, BLOCK, TILE), bf16),
            pltpu.VMEM((2, 2, passages, passage_rows, width), bf16),
            pltpu.VMEM((3, 2, 3, heads) + square, f32),
            pltpu.VMEM((3, 2, 3, heads, 8, TILE), f32),
            pltpu.VMEM((chips, heads, tiles) + square, f32),
            pltpu.VMEM((chips, heads, tiles, TILE), f32),
            pltpu.VMEM((far + 1, heads, tiles) + square, bf16),
            pltpu.VMEM((far + 1, heads, tiles, TILE), f32),
            pltpu.VMEM((near + 1, heads, tiles) + square, bf16),
            pltpu.VMEM((near + 1, heads, tiles, TILE), f32),
            pltpu.VMEM((2, 2, heads, tiles, TILE), f32),
            pltpu.VMEM((tiles, heads) + square, f32),
            pltpu.VMEM((tiles, heads) + square, f32),
            pltpu.VMEM((tiles, heads) + square, f32),
            pltpu.VMEM((tiles, 8, TILE), f32),
            pltpu.VMEM((tiles, TILE, 8), f32),
            pltpu.VMEM((tiles, heads, TILE), f32),
            pltpu.VMEM((heads,) + square, f32),
            pltpu.VMEM((heads,) + square, f32),
            pltpu.VMEM((heads,) + square, f32),
            pltpu.VMEM((heads,) + square, f32),
            pltpu.VMEM((tiles, heads) + square, f32),
            pltpu.SemaphoreType.DMA((6 + 2 * tiles,)),
            pltpu.SemaphoreType.DMA((2, far, 2 * heads + 1)),
            pltpu.SemaphoreType.DMA((2, far, 2 * heads + 1)),
            pltpu.SemaphoreType.DMA((2, far, 3 * heads)),
            pltpu.SemaphoreType.DMA((2, far, 3 * heads)),
            pltpu.SemaphoreType.DMA((2,)),
            pltpu.SemaphoreType.DMA((2,)),
            pltpu.SemaphoreType.DMA((2, 3)),
            pltpu.SemaphoreType.DMA((8,)),
        ],
        compiler_params=pltpu.CompilerParams(
            collective_id=0, has_side_effects=True, vmem_limit_bytes=60 * 1024 * 1024
        ),
    )(
        tokens,
        flat_store,
        retrieval_query_weight,
        passage_key_weight,
        passage_value_weight,
        mixer_query_weight,
        mixer_key_weight,
        mixer_value_weight,
        owners.T,
        entries.T,
        strength_weight.T,
        decay_weight.T,
        retrieval_gate_weight.T,
        forget,
        head_decay_rate[None, :],
        output_norm_gain[None, :],
    )


def solution(mesh):
    return jax.shard_map(
        per_device,
        mesh=mesh,
        in_specs=(
            P(("grp", "st"), None),
            P(("grp", "st"), None),
            P(("grp", "st"), None),
            P(("grp", "st"), None, None),
            P(None, "tp"),
            P(None, "tp"),
            P(None, "tp"),
            P(None, "tp"),
            P(None, "tp"),
            P("tp"),
            P(("grp", "st"), "tp"),
            P(),
            P(None, "tp"),
            P(None, "tp"),
            P(None, "tp"),
            P(None, "tp"),
        ),
        out_specs=P(("grp", "st"), "tp"),
        check_vma=False,
    )
```

```python
import functools

import jax
import jax.numpy as jnp
from jax import lax
from jax.experimental import pallas as pl
from jax.experimental.pallas import tpu as pltpu
from jax.sharding import PartitionSpec as P

MESH = pl.DeviceIdType.MESH
EPS = 1e-06
NEVER = -1e30
BLOCK = 64
TILE = 128
NN = (((1,), (0,)), ((), ()))
NT = (((1,), (1,)), ((), ()))
TN = (((0,), (0,)), ((), ()))


def dot(left, right, dims=NN):
    return lax.dot_general(left, right, dims, preferred_element_type=jnp.float32)


def bdot(left, right, dims=NN):
    return dot(left.astype(jnp.bfloat16), right.astype(jnp.bfloat16), dims)


def rounded(array):
    return array.astype(jnp.bfloat16).astype(jnp.float32)


def kernel(
    chips,
    tok_h,
    store_h,
    wrq_h,
    wpk_h,
    wpv_h,
    wq_h,
    wk_h,
    wv_h,
    owners_h,
    entries_h,
    strength_h,
    decay_h,
    gate_h,
    forget_h,
    rate_h,
    gain_h,
    out,
    owners,
    entries,
    strength,
    decay,
    gate,
    forget,
    rate,
    gain,
    tok,
    store,
    wts,
    qall,
    meta,
    smeta,
    held,
    kv,
    slot,
    slot_l,
    part,
    part_l,
    ret1,
    ret1_l,
    ret2,
    ret2_l,
    fac,
    qn,
    kn,
    vn,
    rows,
    cols,
    rgate,
    power,
    inverse,
    within,
    state,
    normed,
    load_sem,
    q_send,
    q_recv,
    r_send,
    r_recv,
    kv_send,
    kv_recv,
    sm_sem,
    in_sem,
):
    far = chips // 2
    near = chips - 1 - far
    me = lax.axis_index("st")
    core = lax.rem(me, 2)
    chip = lax.div(me, 2)
    sign = 1 - 2 * core
    ahead = lax.rem(chip + sign + chips, chips) * 2 + core
    behind = lax.rem(chip - sign + chips, chips) * 2 + core
    peer = me + sign
    tiles = tok.shape[0] // TILE
    heads = slot.shape[3]
    chunks = 2 * heads
    some = qall.shape[2] // 2
    few = tiles // 2
    scale = TILE ** (-0.5)
    column = (me, peer)
    members = 2 * chips

    tok_rows = tok.shape[0] // tiles
    store_rows = store.shape[0] // tiles

    def load_w(index, ref):
        return pltpu.make_async_copy(ref, wts.at[index], load_sem.at[index])

    def load_tok(t):
        span = pl.ds(t * tok_rows, tok_rows)
        return pltpu.make_async_copy(tok_h.at[span], tok.at[span], load_sem.at[6 + t])

    def load_store(t):
        span = pl.ds(t * store_rows, store_rows)
        return pltpu.make_async_copy(
            store_h.at[span], store.at[span], load_sem.at[6 + tiles + t]
        )

    small = [
        pltpu.make_async_copy(src, dst, in_sem.at[index])
        for index, (src, dst) in enumerate(
            (
                (owners_h, owners),
                (entries_h, entries),
                (strength_h, strength),
                (decay_h, decay),
                (gate_h, gate),
                (forget_h, forget),
                (rate_h, rate),
                (gain_h, gain),
            )
        )
    ]
    for copy in small[:2]:
        copy.start()
    load_w(0, wrq_h).start()
    for t in range(tiles // 2):
        load_tok(t).start()
    barrier = pltpu.get_barrier_semaphore()
    for other in (ahead, behind, peer):
        pl.semaphore_signal(barrier, inc=1, device_id={"st": other}, device_id_type=MESH)

    lane = lax.broadcasted_iota(jnp.int32, (1, TILE), 1)
    count = jnp.zeros((1, TILE), jnp.int32)
    picks = [jnp.zeros((1, TILE), jnp.int32) for _ in range(4)]
    ranks = []
    for copy in small[:2]:
        copy.wait()
    for b in range(8):
        hit = jnp.zeros((1, TILE), jnp.int32)
        entry = jnp.zeros((1, TILE), jnp.int32)
        for i in range(owners.shape[0]):
            same = lane == owners[i, b]
            hit = jnp.where(same, 1, hit)
            entry = jnp.where(same, entries[i, b], entry)
        ranks.append(jnp.where(hit > 0, jnp.minimum(count, 2), 2))
        for r in range(2):
            chosen = (hit > 0) & (count == r)
            picks[2 * r] = jnp.where(chosen, b, picks[2 * r])
            picks[2 * r + 1] = jnp.where(chosen, entry, picks[2 * r + 1])
        count = count + hit
    beside = TILE // members
    for line, values in enumerate((ranks[:beside], ranks[beside:], picks)):
        row = values[0]
        for at in range(1, beside):
            moved = pltpu.roll(values[at], at * members, 1)
            row = jnp.where(lane < at * members, row, moved)
        meta[0, line : line + 1, :] = row
    meta[0, 3:4, :] = count

    def q_copy(way, k, c):
        if way == 0:
            source, target, device = k - 1, k, ahead
        else:
            source, target, device = jnp.where(k == 1, 0, far + k - 1), far + k, behind
        if c == chunks:
            src, dst = meta.at[source], meta.at[target]
        else:
            span = pl.ds(c % 2 * some, some)
            src, dst = qall.at[source, c // 2, span], qall.at[target, c // 2, span]
        return pltpu.make_async_remote_copy(
            src_ref=src,
            dst_ref=dst,
            send_sem=q_send.at[way, k - 1, c],
            recv_sem=q_recv.at[way, k - 1, c],
            device_id={"st": device},
            device_id_type=MESH,
        )

    def r_copy(way, i, c):
        ref, ref_l = ((ret1, ret1_l), (ret2, ret2_l))[way]
        if c >= chunks:
            src, dst = ref_l.at[i, c - chunks], ref_l.at[i + 1, c - chunks]
        else:
            span = pl.ds(c % 2 * few, few)
            src, dst = ref.at[i, c // 2, span], ref.at[i + 1, c // 2, span]
        return pltpu.make_async_remote_copy(
            src_ref=src,
            dst_ref=dst,
            send_sem=r_send.at[way, i, c],
            recv_sem=r_recv.at[way, i, c],
            device_id={"st": (behind, ahead)[way]},
            device_id_type=MESH,
        )

    def kv_copy(which):
        return pltpu.make_async_remote_copy(
            src_ref=kv.at[0, which],
            dst_ref=kv.at[1, which],
            send_sem=kv_send.at[which],
            recv_sem=kv_recv.at[which],
            device_id={"st": peer},
            device_id_type=MESH,
        )

    def sm_copy(way, index, slot_index):
        return pltpu.make_async_copy(
            meta.at[index], smeta.at[way, slot_index], sm_sem.at[way, slot_index]
        )

    load_w(0, wrq_h).wait()
    for t in range(tiles // 2, tiles):
        load_tok(t).start()
    pl.semaphore_wait(barrier, 3)
    for way in range(2):
        q_copy(way, 1, chunks).start()
    for t in range(tiles):
        load_tok(t).wait()
        own = dot(tok[t * tok_rows : (t + 1) * tok_rows, :], wts[0]).astype(jnp.bfloat16)
        for h in range(heads):
            one = own[:, h * TILE : (h + 1) * TILE]
            qall[0, h, 2 * t : 2 * t + 2] = one.reshape(2, BLOCK, TILE)
        if t == tiles // 2:
            for way in range(2):
                q_copy(way, 1, 0).start()

    slot[:, :, 2] = jnp.zeros(slot.shape[:2] + slot.shape[3:], slot.dtype)
    slot_l[:, :, 2] = jnp.full(slot_l.shape[:2] + slot_l.shape[3:], NEVER, jnp.float32)
    state[...] = jnp.zeros_like(state)
    for c in range(1, chunks):
        for way in range(2):
            q_copy(way, 1, c).start()
    load_w(1, wpk_h).start()
    load_w(2, wpv_h).start()
    for t in range(tiles):
        load_store(t).start()
    for copy in small[2:]:
        copy.start()

    group = kv.shape[2] // tiles

    def project_passages(t):
        load_store(t).wait()
        piece = store[pl.ds(t * store_rows, store_rows), :]
        for which in range(2):
            made = dot(piece, wts[1 + which]).astype(jnp.bfloat16)
            kv[0, which, pl.ds(t * group, group)] = made.reshape(group, BLOCK, made.shape[1])

    def forward(k, c):
        last_far = isinstance(k, int) and k >= far
        q_copy(0, k, c).wait_recv()
        if not last_far:
            q_copy(0, k + 1, c).start()
            q_copy(1, k, c).wait_recv()

            @pl.when(k < near)
            def _():
                q_copy(1, k + 1, c).start()

    row_i = lax.broadcasted_iota(jnp.int32, (TILE, TILE), 0)
    col_i = lax.broadcasted_iota(jnp.int32, (TILE, TILE), 1)
    first_half = lax.broadcasted_iota(jnp.int32, (1, TILE), 1) < BLOCK

    def project_tokens(t):
        rates = jnp.where(
            lax.broadcasted_iota(jnp.int32, (heads, TILE), 0) == 0, rate[0:1, 0:1], rate[0:1, 1:2]
        )
        piece = tok[t * tok_rows : (t + 1) * tok_rows, :]
        for index, ref in ((3, qn), (4, kn), (5, vn)):
            made = rounded(dot(piece, wts[index]))
            for h in range(heads):
                one = made[:, h * TILE : (h + 1) * TILE]
                if index < 5:
                    one = one * lax.rsqrt(jnp.sum(one * one, axis=1, keepdims=True) + EPS)
                if index == 3:
                    one = one * scale
                ref[t, h] = one
        small_w = jnp.concatenate(
            [strength[...], decay[...], gate[...], jnp.zeros((2, tok.shape[1]), tok.dtype)], axis=0
        )
        gates = jnp.transpose(dot(piece, small_w, NT))
        beta = jax.nn.sigmoid(gates[0:2, :])
        raw = gates[2:4, :]
        soft = jnp.maximum(raw, 0.0) + jnp.log1p(jnp.exp(-jnp.abs(raw)))
        cumul = -rates * soft + forget[t]
        spot = lax.broadcasted_iota(jnp.int32, cumul.shape, 1)
        shift = 1
        while shift < TILE:
            cumul = cumul + jnp.where(spot >= shift, pltpu.roll(cumul, shift, 1), 0.0)
            shift *= 2
        tail = jnp.exp(cumul[:, TILE - 1 : TILE] - cumul)
        lines = jnp.concatenate([cumul, jnp.exp(cumul), tail, beta], axis=0)
        rows[t] = lines
        cols[t] = jnp.transpose(lines)
        rgate[t] = jax.nn.sigmoid(gates[4:6, :])

    def attend(spot, way, parity, j, r, which):
        block = smeta[way, parity, 2, 2 * r * members + column[j]]
        passage = smeta[way, parity, 2, (2 * r + 1) * members + column[j]]
        for h in which:
            span = slice(h * TILE, (h + 1) * TILE)
            query = held[spot, h, block]
            query = jnp.concatenate([query, query], axis=0)
            scores = dot(kv[j, 0, passage, :, span], query, NT) * scale
            peak = jnp.max(scores, axis=0, keepdims=True)
            expo = jnp.exp(scores - peak)
            total = jnp.sum(expo, axis=0, keepdims=True)
            weights = (expo / total).astype(jnp.bfloat16)
            slot[spot, j, r, h] = dot(kv[j, 1, passage, :, span], weights, TN)
            slot_l[spot, j, r, h] = jnp.broadcast_to(peak + jnp.log(total), (8, TILE))

    def assemble(s, spot, way, parity, which):
        for t in range(tiles):
            picks = [
                [
                    smeta[way, parity, b // beside, b % beside * members + column[j]]
                    for b in (2 * t, 2 * t + 1)
                ]
                for j in range(2)
            ]
            for h in which:
                logs = [
                    jnp.where(
                        first_half,
                        slot_l[spot, j, picks[j][0], h, 0:1, :],
                        slot_l[spot, j, picks[j][1], h, 0:1, :],
                    )
                    for j in range(2)
                ]
                peak = jnp.maximum(logs[0], logs[1])
                shares = [jnp.exp(one - peak) for one in logs]
                total = shares[0] + shares[1]
                made = 0.0
                for j in range(2):
                    both = jnp.where(
                        first_half,
                        slot[spot, j, picks[j][0], h],
                        slot[spot, j, picks[j][1], h],
                    )
                    made = made + both * (shares[j] / total)
                part[s, h, t] = made
                part_l[s, h, t : t + 1, :] = peak + jnp.log(total)

    def delta(t, stage):
        ident = jnp.where(row_i == col_i, 1.0, 0.0)
        for h in range(heads):
            if stage == 0:
                lower = row_i >= col_i
                spread = cols[t, :, h : h + 1] - rows[t, h : h + 1, :]
                damping = jnp.where(lower, jnp.exp(jnp.where(lower, spread, 0.0)), 0.0)
                keys = kn[t, h]
                k_beta = keys * cols[t, :, 6 + h : 7 + h]
                inner = jnp.where(row_i > col_i, bdot(k_beta, keys, NT) * damping, 0.0)
                within[h] = jnp.where(lower, bdot(qn[t, h], keys, NT) * damping, 0.0)
                power[h] = inner
                inverse[h] = ident - inner
            elif stage < 3:
                value, made = power[h], inverse[h]
                for _ in range(3):
                    value = bdot(value, value)
                    made = bdot(made, ident + value)
                power[h] = value
                inverse[h] = made
            else:
                beta = cols[t, :, 6 + h : 7 + h]
                grown = cols[t, :, 2 + h : 3 + h]
                keys = kn[t, h]
                made = inverse[h]
                now = state[h]
                base = bdot(made, vn[t, h] * beta)
                mix = bdot(made, keys * beta * grown)
                fresh = base - bdot(mix, now)
                result = bdot(qn[t, h] * grown, now) + bdot(within[h], fresh)
                tail = keys * cols[t, :, 4 + h : 5 + h]
                state[h] = now * grown[TILE - 1 : TILE, :] + bdot(tail, fresh, TN)
                spread = jnp.mean(result * result, axis=1, keepdims=True)
                normed[t, h] = result * lax.rsqrt(spread + EPS) * gain[...]

    every = tuple(range(heads))
    forward(1, chunks)
    for c in range(chunks):
        forward(1, c)
        if c == 0:
            load_w(1, wpk_h).wait()
            load_w(2, wpv_h).wait()
        project_passages(c)
    for index, ref in ((3, wq_h), (4, wk_h), (5, wv_h)):
        load_w(index, ref).start()
    for which in range(2):
        kv_copy(which).start()
    forward(2, chunks)
    for way in range(2):
        sm_copy(way, (2, far + 2)[way], 0).start()
    for c in range(chunks):
        forward(2, c)
        if c == 0:
            for index, ref in ((3, wq_h), (4, wk_h), (5, wv_h)):
                load_w(index, ref).wait()
            for copy in small[2:]:
                copy.wait()
        project_tokens(c)
    for which in range(2):
        kv_copy(which).wait_recv()

    def enter(k, parity):
        forward(k, chunks)
        for way in range(2):
            sm_copy(way, (k, far + k)[way], parity).start()
        for way in range(2):
            sm_copy(way, (k - 1, far + k - 1)[way], 1 - parity).wait()
        for way in range(2):
            held[way] = qall[(k - 1, far + k - 1)[way]]

    def hop(k, carry):
        parity = lax.rem(k, 2)
        before = 1 - parity
        enter(k, parity)
        for c in range(4):
            forward(k, c)
            for way in range(2):
                attend(way, way, before, c // 2, c % 2, every)
        for way in range(2):
            assemble((k - 1, far + k - 1)[way], way, way, before, every)
        return carry

    lax.fori_loop(3, near, hop, 0)

    def whole(s, spot, way, parity, which):
        for h in which:
            held[spot, h] = qall[s, h]
        for c in range(4):
            attend(spot, way, parity, c // 2, c % 2, which)
        assemble(s, spot, way, parity, which)

    def r_begin(way, s, h):
        ref, ref_l = ((ret1, ret1_l), (ret2, ret2_l))[way]
        ref_l[0, h] = part_l[s, h]
        ref[0, h] = part[s, h].astype(jnp.bfloat16)
        for c in (chunks + h, 2 * h, 2 * h + 1):
            r_copy(way, 0, c).start()

    last = near % 2
    before = 1 - last
    enter(near, last)
    sm_copy(1, far + near, last).wait()
    for c in range(4):
        forward(near, c)
        for way in range(2):
            attend(way, way, before, c // 2, c % 2, every)
        if c % 2:
            whole(far + near, 2, 1, last, (c // 2,))
            r_begin(1, far + near, c // 2)
    q_copy(0, far, chunks).wait_recv()
    sm_copy(0, far, 2).start()
    sm_copy(1, far + 1, last).start()
    sm_copy(0, near, last).wait()
    sm_copy(0, far, 2).wait()
    for h in range(heads):
        q_copy(0, far, 2 * h).wait_recv()
        q_copy(0, far, 2 * h + 1).wait_recv()
        whole(far, 2, 0, 2, (h,))
        r_begin(0, far, h)
        if h == 0:
            for way in range(2):
                assemble((near - 1, far + near - 1)[way], way, way, before, every)
            sm_copy(1, 0, before).start()
            sm_copy(0, 1, before).start()
        whole(near, 0, 0, last, (h,))
    sm_copy(1, far + 1, last).wait()
    sm_copy(1, 0, before).wait()
    sm_copy(0, 1, before).wait()

    def meet_logs(way, i, s, h):
        ref_l = (ret1_l, ret2_l)[way]
        r_copy(way, i - 1, chunks + h).wait_recv()
        theirs, mine = ref_l[i, h], part_l[s, h]
        peak = jnp.maximum(theirs, mine)
        shares = jnp.exp(theirs - peak), jnp.exp(mine - peak)
        total = shares[0] + shares[1]
        fac[way, 0, h] = shares[0] / total
        fac[way, 1, h] = shares[1] / total
        ref_l[i, h] = peak + jnp.log(total)

    def meet(way, i, s, c):
        ref = (ret1, ret2)[way]
        h = c // 2
        r_copy(way, i - 1, c).wait_recv()
        for t in range(c % 2 * few, c % 2 * few + few):
            made = ref[i, h, t].astype(jnp.float32) * fac[way, 0, h, t : t + 1, :]
            made = made + part[s, h, t] * fac[way, 1, h, t : t + 1, :]
            ref[i, h, t] = made.astype(jnp.bfloat16)

    def back(i, carry):
        pair = far - i, far + near - i
        for c in range(chunks):
            for way in (1, 0):
                if c % 2 == 0:
                    meet_logs(way, i, pair[way], c // 2)
                meet(way, i, pair[way], c)
                if c % 2 == 0:
                    r_copy(way, i, chunks + c // 2).start()
                r_copy(way, i, c).start()

            @pl.when(i <= tiles)
            def _():
                delta(i - 1, c)

        @pl.when(i <= 3)
        def _():
            way = i % 2
            index = jnp.where(i == 1, far + 1, jnp.where(i == 2, 1, 0))
            whole(index, 0, way, jnp.where(i == 1, last, before), every)

        return carry

    lax.fori_loop(1, near, back, 0)
    for c in range(chunks):
        if c % 2 == 0:
            meet_logs(0, near, far - near, c // 2)
        meet(0, near, far - near, c)
        if c % 2:
            r_copy(0, near, chunks + c // 2).start()
            r_copy(0, near, c - 1).start()
            r_copy(0, near, c).start()

    for h in range(heads):
        span = slice(h * TILE, (h + 1) * TILE)
        r_copy(1, near - 1, chunks + h).wait_recv()
        r_copy(0, far - 1, chunks + h).wait_recv()
        logs = part_l[0, h], ret1_l[far, h], ret2_l[near, h]
        peak = jnp.maximum(jnp.maximum(logs[0], logs[1]), logs[2])
        shares = [jnp.exp(one - peak) for one in logs]
        total = shares[0] + shares[1] + shares[2]
        shares = [one / total for one in shares]
        for t in range(tiles):
            if t % few == 0:
                r_copy(1, near - 1, 2 * h + t // few).wait_recv()
                r_copy(0, far - 1, 2 * h + t // few).wait_recv()
            made = part[0, h, t] * shares[0][t : t + 1, :]
            made = made + ret1[far, h, t].astype(jnp.float32) * shares[1][t : t + 1, :]
            made = made + ret2[near, h, t].astype(jnp.float32) * shares[2][t : t + 1, :]
            made = jnp.transpose(made * rgate[t, h : h + 1, :])
            out[t * TILE : (t + 1) * TILE, span] = (normed[t, h] + made).astype(out.dtype)

    for which in range(2):
        kv_copy(which).wait_send()
    for way in range(2):
        hops = (far, near)[way]

        def drain(i, carry, way=way):
            for c in range(chunks + 1):
                q_copy(way, i + 1, c).wait_send()
            for c in range(chunks + heads):
                r_copy(way, i, c).wait_send()
            return carry

        lax.fori_loop(0, hops, drain, 0)


def per_device(
    tokens,
    owners,
    entries,
    store,
    mixer_query_weight,
    mixer_key_weight,
    mixer_value_weight,
    strength_weight,
    decay_weight,
    head_decay_rate,
    extra_forgetting_exponent,
    output_norm_gain,
    retrieval_query_weight,
    passage_key_weight,
    passage_value_weight,
    retrieval_gate_weight,
):
    heads = head_decay_rate.shape[0]
    length, model = tokens.shape
    width = mixer_query_weight.shape[1]
    blocks = owners.shape[0]
    passages, passage_rows = store.shape[:2]
    tiles = length // TILE
    chips = lax.axis_size("st") // 2
    far = chips // 2
    near = chips - 1 - far
    flat_store = store.reshape(passages * passage_rows, model)
    forget = extra_forgetting_exponent.reshape(tiles, TILE, heads).transpose(0, 2, 1)
    any_spec = pl.BlockSpec(memory_space=pl.ANY)
    vmem_spec = pl.BlockSpec(memory_space=pltpu.VMEM)
    f32, bf16 = jnp.float32, jnp.bfloat16
    square = (TILE, TILE)
    return pl.pallas_call(
        functools.partial(kernel, chips),
        out_shape=pltpu.VMEM((length, width), bf16),
        in_specs=[any_spec] * 16,
        out_specs=vmem_spec,
        scratch_shapes=[
            pltpu.SMEM((owners.shape[1], blocks), jnp.int32),
            pltpu.SMEM((owners.shape[1], blocks), jnp.int32),
            pltpu.VMEM((heads, model), bf16),
            pltpu.VMEM((heads, model), bf16),
            pltpu.VMEM((heads, model), bf16),
            pltpu.VMEM((tiles, heads, TILE), f32),
            pltpu.VMEM((1, heads), f32),
            pltpu.VMEM((1, TILE), f32),
            pltpu.VMEM((length, model), bf16),
            pltpu.VMEM((passages * passage_rows, model), bf16),
            pltpu.VMEM((6, model, width), bf16),
            pltpu.VMEM((chips, heads, blocks, BLOCK, TILE), bf16),
            pltpu.VMEM((chips, 4, TILE), jnp.int32),
            pltpu.SMEM((2, 3, 4, TILE), jnp.int32),
            pltpu.VMEM((3, heads, blocks, BLOCK, TILE), bf16),
            pltpu.VMEM((2, 2, passages, passage_rows, width), bf16),
            pltpu.VMEM((3, 2, 3, heads) + square, f32),
            pltpu.VMEM((3, 2, 3, heads, 8, TILE), f32),
            pltpu.VMEM((chips, heads, tiles) + square, f32),
            pltpu.VMEM((chips, heads, tiles, TILE), f32),
            pltpu.VMEM((far + 1, heads, tiles) + square, bf16),
            pltpu.VMEM((far + 1, heads, tiles, TILE), f32),
            pltpu.VMEM((near + 1, heads, tiles) + square, bf16),
            pltpu.VMEM((near + 1, heads, tiles, TILE), f32),
            pltpu.VMEM((2, 2, heads, tiles, TILE), f32),
            pltpu.VMEM((tiles, heads) + square, f32),
            pltpu.VMEM((tiles, heads) + square, f32),
            pltpu.VMEM((tiles, heads) + square, f32),
            pltpu.VMEM((tiles, 8, TILE), f32),
            pltpu.VMEM((tiles, TILE, 8), f32),
            pltpu.VMEM((tiles, heads, TILE), f32),
            pltpu.VMEM((heads,) + square, f32),
            pltpu.VMEM((heads,) + square, f32),
            pltpu.VMEM((heads,) + square, f32),
            pltpu.VMEM((heads,) + square, f32),
            pltpu.VMEM((tiles, heads) + square, f32),
            pltpu.SemaphoreType.DMA((6 + 2 * tiles,)),
            pltpu.SemaphoreType.DMA((2, far, 2 * heads + 1)),
            pltpu.SemaphoreType.DMA((2, far, 2 * heads + 1)),
            pltpu.SemaphoreType.DMA((2, far, 3 * heads)),
            pltpu.SemaphoreType.DMA((2, far, 3 * heads)),
            pltpu.SemaphoreType.DMA((2,)),
            pltpu.SemaphoreType.DMA((2,)),
            pltpu.SemaphoreType.DMA((2, 3)),
            pltpu.SemaphoreType.DMA((8,)),
        ],
        compiler_params=pltpu.CompilerParams(
            collective_id=0, has_side_effects=True, vmem_limit_bytes=60 * 1024 * 1024
        ),
    )(
        tokens,
        flat_store,
        retrieval_query_weight,
        passage_key_weight,
        passage_value_weight,
        mixer_query_weight,
        mixer_key_weight,
        mixer_value_weight,
        owners.T,
        entries.T,
        strength_weight.T,
        decay_weight.T,
        retrieval_gate_weight.T,
        forget,
        head_decay_rate[None, :],
        output_norm_gain[None, :],
    )


def solution(mesh):
    return jax.shard_map(
        per_device,
        mesh=mesh,
        in_specs=(
            P(("grp", "st"), None),
            P(("grp", "st"), None),
            P(("grp", "st"), None),
            P(("grp", "st"), None, None),
            P(None, "tp"),
            P(None, "tp"),
            P(None, "tp"),
            P(None, "tp"),
            P(None, "tp"),
            P("tp"),
            P(("grp", "st"), "tp"),
            P(),
            P(None, "tp"),
            P(None, "tp"),
            P(None, "tp"),
            P(None, "tp"),
        ),
        out_specs=P(("grp", "st"), "tp"),
        check_vma=False,
    )
```
